128 devices in a mesh: sp: 64 (over z, y, x), tp: 2 (over core).
Axes of the slice: x: 4, y: 4, z: 4, core: 2. Of those that a mesh axis runs over, the one named last changes fastest.
Arguments:
- residual: bfloat16 [16384, 2048], P(('sp', 'tp')), may hold values from -6 to 6
- queries: bfloat16 [16384, 512], P('sp', 'tp'), may hold values from -6 to 6
- key_rows: bfloat16 [16384, 512], P('sp', 'tp'), may hold values from -6 to 6
- value_rows: bfloat16 [16384, 1024], P('sp', 'tp'), may hold values from -6 to 6
- out_gate: bfloat16 [16384, 1024], P('sp', 'tp'), may hold values from -6 to 6
- gate_logits: bfloat16 [16384, 512], P('sp', 'tp')
- head_gain: float32 [128], replicated, may hold values from 0.1 to 1.9
- out_weight: bfloat16 [1024, 2048], replicated, may hold values from -0.1875 to 0.1875
- norm_gain: float32 [2048], replicated, may hold values from 0.1 to 1.9
- routes: int32 [16384, 2], P(('sp', 'tp')), may hold values from 0 to 127, as said below
- group_score: float32 [16384], P(('sp', 'tp')), may hold values from 0.25 to 1
- expert_score: float32 [16384, 2], P(('sp', 'tp')), may hold values from 0.1 to 1
- gate_weight: bfloat16 [128, 2048, 512], P(('sp', 'tp')), may hold values from -0.125 to 0.125
- up_weight: bfloat16 [128, 2048, 512], P(('sp', 'tp')), may hold values from -0.125 to 0.125
- down_weight: bfloat16 [128, 512, 2048], P(('sp', 'tp')), may hold values from -0.25 to 0.25
Outputs:
- layer_out: bfloat16 [16384, 2048], P(('sp', 'tp'))
The draws below stay inside these ranges and needn't reach their ends.
Inputs may be any that keep to these rules, and one draw needn't show every extreme that they name: `routes`: the two experts of a token differ and lie in one group of 8 consecutive expert numbers. In each aligned block of 128 tokens (the tokens of one device) no expert is named more than 3 times, and one expert, the same for all blocks of a draw, is named exactly 3 times in every block.
All inputs are finite; a program needn't handle non-finite values.
Results may differ from the reference program's by a relative error of at most 0.0056.
Values may be sent and summed in bfloat16 or wider, within the bound.
A program may use at most 64 MiB of HBM per device.

```python
import math
from functools import partial
import jax
import jax.numpy as jnp
from jax import lax

MODEL_WIDTH = 2048
HEADS = 8
KEY_DIM = 64
VALUE_DIM = 128
EXPERT_WIDTH = 512
GROUP_SIZE = 8
BLOCK = 64
SEGMENT = 256
KEYS = 512
VALUES = 1024
ROWS = 128
TOKENS = 16384
EXPERTS = 128
GROUPS = 16
CAPACITY = 3


def draw_gate_logits(key, part):
    subkeys = jax.random.split(key, 7)
    slow_share = 0.5
    slow_heads = jax.random.bernoulli(subkeys[0], slow_share, (HEADS,))
    chain_loss = jnp.exp(jax.random.uniform(subkeys[1], (HEADS, KEY_DIM), jnp.float32, jnp.log(0.2), jnp.log(0.8)))
    slow_logit = jnp.log(TOKENS / (16.0 * chain_loss))
    fast_rate = jnp.exp(jax.random.uniform(subkeys[2], (HEADS, KEY_DIM), jnp.float32, jnp.log(1.0 / 100.0), jnp.log(1.0 / 30.0)))
    fast_logit = -jnp.log(jnp.expm1(16.0 * fast_rate))
    base_logit = jnp.where(slow_heads[:, None], slow_logit, fast_logit)
    jitter = jax.random.uniform(subkeys[3], (TOKENS, HEADS, KEY_DIM), jnp.float32, -1.0, 1.0)
    offset = jax.random.uniform(subkeys[4], (TOKENS // SEGMENT, HEADS), jnp.float32, -0.7, 0.7)
    offset = jnp.repeat(offset, SEGMENT, axis=0)
    router_scores = base_logit[None] + jitter + offset[:, :, None]
    slot_places = jax.random.randint(subkeys[5], (2, HEADS), 0, TOKENS)
    spike_strength = jax.random.uniform(subkeys[6], (2, HEADS), jnp.float32, -11.0, -4.0)
    token_position = jnp.arange(TOKENS, dtype=jnp.int32)[:, None]
    spike_value = jnp.where(token_position == slot_places[0][None, :], spike_strength[0][None, :], spike_strength[1][None, :])
    spike_mask = (token_position == slot_places[0][None, :]) | (token_position == slot_places[1][None, :])
    router_scores = jnp.where(spike_mask[:, :, None], spike_value[:, :, None], router_scores)
    return router_scores.reshape(TOKENS, HEADS * KEY_DIM).astype(jnp.bfloat16)


def shuffle_group(group_key):
    return jax.random.permutation(group_key, GROUP_SIZE).astype(jnp.int32)


def route_block(block_key, hot_expert):
    subkeys = jax.random.split(block_key, 4)
    slot_total = GROUPS * 3 * CAPACITY
    labels = (jax.random.permutation(subkeys[0], slot_total) // (3 * CAPACITY)).astype(jnp.int32)
    chosen = labels[:5 * ROWS // 8]
    group_index = jnp.arange(GROUPS, dtype=jnp.int32)
    extra_count = jnp.sum((chosen[:, None] == group_index[None, :]).astype(jnp.int32), axis=0)
    tickets = 2 * CAPACITY + 2 * extra_count
    group_rows = tickets // 2
    hot_group = hot_expert // GROUP_SIZE
    hot_local = hot_expert % GROUP_SIZE
    orders = jax.vmap(shuffle_group)(jax.random.split(subkeys[1], GROUPS))
    rank_grid = jnp.arange(GROUP_SIZE, dtype=jnp.int32)[None, :]
    hot_row = (group_index == hot_group)[:, None]
    sort_key = jnp.where(hot_row & (orders == hot_local), -1, rank_grid)
    orders = jnp.take_along_axis(orders, jnp.argsort(sort_key, axis=1, stable=True), axis=1)
    remaining = tickets[:, None] - CAPACITY
    hot_counts = jnp.where(rank_grid == 0, CAPACITY, remaining // (GROUP_SIZE - 1) + (rank_grid - 1 < remaining % (GROUP_SIZE - 1)).astype(jnp.int32))
    drawn_counts = tickets[:, None] // GROUP_SIZE + (rank_grid < tickets[:, None] % GROUP_SIZE).astype(jnp.int32)
    counts = jnp.where(hot_row, hot_counts, drawn_counts)
    count_ends = jnp.cumsum(counts, axis=1)
    row_ends = jnp.cumsum(group_rows)
    row_ids = jnp.arange(ROWS, dtype=jnp.int32)
    group_of = jnp.sum((row_ids[:, None] >= row_ends[None, :]).astype(jnp.int32), axis=1)
    start_of = row_ends[group_of] - group_rows[group_of]
    first_pos = row_ids - start_of
    second_pos = first_pos + group_rows[group_of]
    ends_table = count_ends[group_of]
    first_rank = jnp.sum((first_pos[:, None] >= ends_table).astype(jnp.int32), axis=1)
    second_rank = jnp.sum((second_pos[:, None] >= ends_table).astype(jnp.int32), axis=1)
    order_rows = orders[group_of]
    first_expert = group_of * GROUP_SIZE + jnp.take_along_axis(order_rows, first_rank[:, None], axis=1)[:, 0]
    second_expert = group_of * GROUP_SIZE + jnp.take_along_axis(order_rows, second_rank[:, None], axis=1)[:, 0]
    expert_pairs = jnp.stack([first_expert, second_expert], axis=1)
    flip_order = jax.random.randint(subkeys[2], (ROWS,), 0, 2)
    expert_pairs = jnp.where(flip_order[:, None] == 1, expert_pairs[:, ::-1], expert_pairs)
    shuffled = expert_pairs[jax.random.permutation(subkeys[3], ROWS)]
    return shuffled.astype(jnp.int32)


def draw_routes(key, part):
    hot_expert = jax.random.randint(jax.random.fold_in(key, 11), (), 0, EXPERTS)
    block_keys = jax.random.split(jax.random.fold_in(key, 12), TOKENS // ROWS)
    blocks_out = jax.vmap(partial(route_block, hot_expert=hot_expert))(block_keys)
    return blocks_out.reshape(TOKENS, 2).astype(jnp.int32)


def block_scale(stream_key, dims, cuts, smallest, top_value):
    factor_of = 1.0
    for position, blocks in cuts:
        steps = jax.random.uniform(jax.random.fold_in(jax.random.fold_in(stream_key, 6), position), (blocks,), jnp.float32, smallest / len(cuts), top_value / len(cuts))
        factor_of = factor_of * jnp.repeat(jnp.exp(steps), dims[position] // blocks).reshape((-1,) + (1,) * (len(dims) - 1 - position))
    return factor_of


def gaussian(key, dims, spread, reach, cuts=(), held_as=jnp.bfloat16):
    drawn = jax.random.normal(key, dims, jnp.float32) * spread
    if len(cuts) > 0:
        drawn = block_scale(key, dims, cuts, -0.22, 0.18) * drawn
    return jnp.clip(drawn, min=-reach, max=reach).astype(held_as)


def setup_inputs(seed: int = 0) -> dict:
    arg_keys = jax.random.split(jax.random.key(seed), 16)
    residual = gaussian(arg_keys[0], (TOKENS, MODEL_WIDTH), 1.0, 6.0, ((0, 128),))
    queries = gaussian(arg_keys[1], (TOKENS, KEYS), 1.0, 6.0, ((0, 64), (1, 2)))
    key_rows = gaussian(arg_keys[2], (TOKENS, KEYS), 1.0, 6.0, ((0, 64), (1, 2)))
    value_rows = gaussian(arg_keys[3], (TOKENS, VALUES), 1.0, 6.0, ((0, 64), (1, 2)))
    out_gate = gaussian(arg_keys[4], (TOKENS, VALUES), 1.0, 6.0, ((0, 64), (1, 2)))
    gate_logits = draw_gate_logits(jax.random.fold_in(arg_keys[15], 71), 0)
    head_gain = jnp.clip(1.0 + 0.18 * jax.random.normal(arg_keys[6], (VALUE_DIM,), jnp.float32), 0.1, 1.9)
    out_weight = gaussian(arg_keys[7], (VALUES, MODEL_WIDTH), VALUES ** -0.5, 0.1875)
    norm_gain = jnp.clip(1.0 + 0.18 * jax.random.normal(arg_keys[8], (MODEL_WIDTH,), jnp.float32), 0.1, 1.9)
    routes = draw_routes(jax.random.fold_in(arg_keys[15], 71), 0)
    group_score = jnp.clip(0.25 + 0.75 * jax.random.uniform(arg_keys[10], (TOKENS,), jnp.float32) ** block_scale(arg_keys[10], (TOKENS,), ((0, 128),), -0.2, 0.2), 0.25, 1.0)
    expert_score = jnp.clip(jnp.exp(math.log(1.0) - 2.3025851 * jax.random.uniform(arg_keys[11], (TOKENS, 2), jnp.float32) ** block_scale(arg_keys[11], (TOKENS, 2), ((0, 128),), -0.2, 0.2)), 0.1, 1.0)
    gate_weight = gaussian(arg_keys[12], (EXPERTS, MODEL_WIDTH, EXPERT_WIDTH), MODEL_WIDTH ** -0.5, 0.125, ((0, 128),))
    up_weight = gaussian(arg_keys[13], (EXPERTS, MODEL_WIDTH, EXPERT_WIDTH), MODEL_WIDTH ** -0.5, 0.125, ((0, 128),))
    down_weight = gaussian(arg_keys[14], (EXPERTS, EXPERT_WIDTH, MODEL_WIDTH), EXPERT_WIDTH ** -0.5, 0.25, ((0, 128),))
    return dict(residual=residual, queries=queries, key_rows=key_rows, value_rows=value_rows, out_gate=out_gate, gate_logits=gate_logits, head_gain=head_gain, out_weight=out_weight, norm_gain=norm_gain, routes=routes, group_score=group_score, expert_score=expert_score, gate_weight=gate_weight, up_weight=up_weight, down_weight=down_weight)


def block_parts(queries, key_rows, value_rows, gate_logits):
    length = queries.shape[0]
    head_count = queries.shape[1] // KEY_DIM
    blocks = length // BLOCK

    def arrange(source, inner_size):
        return source.astype(jnp.float32).reshape(blocks, BLOCK, head_count, inner_size).transpose(0, 2, 1, 3)
    decay_log = jax.nn.log_sigmoid(gate_logits.astype(jnp.float32)) / 16.0
    running = jnp.cumsum(arrange(decay_log, KEY_DIM), axis=2)
    closing = running[:, :, -1:, :]
    query_scaled = arrange(queries, KEY_DIM) * KEY_DIM ** (-0.5) * jnp.exp(running)
    key_float = arrange(key_rows, KEY_DIM)
    key_inverse = key_float * jnp.exp(-running)
    key_closing = key_float * jnp.exp(closing - running)
    value_float = arrange(value_rows, VALUE_DIM)
    causal = jnp.tril(jnp.ones((BLOCK, BLOCK), dtype=bool))
    scores = jnp.where(causal, jnp.einsum('nhcd,nhsd->nhcs', query_scaled, key_inverse, precision=lax.Precision.HIGHEST), 0.0)
    within = jnp.einsum('nhcs,nhsv->nhcv', scores, value_float, precision=lax.Precision.HIGHEST)
    increments = jnp.einsum('nhcd,nhcv->nhdv', key_closing, value_float, precision=lax.Precision.HIGHEST)
    return (query_scaled, within, increments, closing[:, :, 0, :])

def advance(carried, inputs):
    increment, block_log = inputs
    return (jnp.exp(block_log)[..., None] * carried + increment, carried)

def finish(attended, head_gain, out_gate):
    blocks = attended.shape[0]
    head_count = attended.shape[1]
    length = blocks * BLOCK
    ordered = attended.transpose(0, 2, 1, 3).reshape(length, head_count, VALUE_DIM)
    normed = ordered * lax.rsqrt(lax.optimization_barrier(jnp.mean(ordered * ordered, axis=-1, keepdims=True)) + 1e-06) * head_gain
    gating = jax.nn.silu(out_gate.astype(jnp.float32)).reshape(length, head_count, VALUE_DIM)
    return (normed * gating).reshape(length, head_count * VALUE_DIM).astype(jnp.bfloat16)

def route_slots(block_routes, experts_total, capacity):
    row_count = block_routes.shape[0]
    flattened = block_routes.reshape(-1)
    onehot = (flattened[:, None] == jnp.arange(experts_total, dtype=jnp.int32)[None, :]).astype(jnp.int32)
    ranking = lax.optimization_barrier(jnp.sum((jnp.cumsum(onehot, axis=0) - onehot) * onehot, axis=1))
    slot_index = flattened * capacity + ranking
    route_ids = jnp.arange(2 * row_count, dtype=jnp.int32) // 2
    owners = jnp.full((experts_total * capacity,), row_count, jnp.int32).at[slot_index].set(route_ids)
    return (slot_index, owners)

def expert_apply(rows_in, gate_matrix, up_matrix, down_matrix):
    gated = jnp.dot(rows_in, gate_matrix, preferred_element_type=jnp.float32)
    lifted = jnp.dot(rows_in, up_matrix, preferred_element_type=jnp.float32)
    inner_rows = (jax.nn.silu(gated) * lifted).astype(jnp.bfloat16)
    return jnp.dot(inner_rows, down_matrix, preferred_element_type=jnp.float32).astype(jnp.bfloat16)

def reference(residual, queries, key_rows, value_rows, out_gate, gate_logits, head_gain, out_weight, norm_gain, routes, group_score, expert_score, gate_weight, up_weight, down_weight):
    query_scaled, within, increments, block_logs = block_parts(queries, key_rows, value_rows, gate_logits)
    zero_state = jnp.zeros(increments.shape[1:], jnp.float32)
    _, states = lax.scan(advance, zero_state, (increments, block_logs))
    attended = within + jnp.einsum('nhcd,nhdv->nhcv', query_scaled, states, precision=lax.Precision.HIGHEST)
    mixer_out = finish(attended, head_gain, out_gate)
    summed = residual.astype(jnp.float32) + jnp.dot(mixer_out, out_weight, preferred_element_type=jnp.float32)
    merged = summed.astype(jnp.bfloat16)
    widened = lax.optimization_barrier(merged).astype(jnp.float32)
    normed = (widened * lax.rsqrt(lax.optimization_barrier(jnp.mean(widened * widened, axis=-1, keepdims=True)) + 1e-06) * norm_gain).astype(jnp.bfloat16)
    tokens_total = residual.shape[0]
    model_width = residual.shape[1]
    blocks = tokens_total // ROWS
    experts_total = gate_weight.shape[0]
    slot_index, owners = jax.vmap(partial(route_slots, experts_total=experts_total, capacity=CAPACITY))(routes.reshape(blocks, ROWS, 2))
    offsets = (jnp.arange(blocks, dtype=jnp.int32) * ROWS)[:, None]
    sources = jnp.where(owners < ROWS, owners + offsets, tokens_total).astype(jnp.int32)
    padded = jnp.concatenate([normed, jnp.zeros((1, model_width), jnp.bfloat16)], axis=0)
    per_expert = sources.reshape(blocks, experts_total, CAPACITY).transpose(1, 0, 2).reshape(experts_total, blocks * CAPACITY)

    def serve(inputs):
        indices, gate_matrix, up_matrix, down_matrix = inputs
        return expert_apply(padded[indices], gate_matrix, up_matrix, down_matrix)
    results = lax.map(serve, (per_expert, gate_weight, up_weight, down_weight))
    expert_ids = routes.reshape(blocks, 2 * ROWS)
    ranking = slot_index - expert_ids * CAPACITY
    block_base = (jnp.arange(blocks, dtype=jnp.int32) * CAPACITY)[:, None]
    token_position = (expert_ids * (blocks * CAPACITY) + block_base + ranking).astype(jnp.int32)
    picked = results.reshape(-1, model_width)[token_position.reshape(-1)].reshape(tokens_total, 2, model_width)
    weights = group_score[:, None] * expert_score / lax.optimization_barrier(jnp.sum(expert_score, axis=1, keepdims=True))
    combined = weights[:, 0:1] * picked[:, 0].astype(jnp.float32) + weights[:, 1:2] * picked[:, 1].astype(jnp.float32)
    return (widened + combined).astype(jnp.bfloat16)
```

```python
import jax
import jax.numpy as jnp
from jax import lax
from jax.experimental import pallas as pl
from jax.experimental.pallas import tpu as pltpu
from jax.sharding import Mesh
from jax.sharding import PartitionSpec as P

AXES = ("sp_0", "sp_1", "sp_2", "tp")
SP = AXES[:3]
MESH = pl.DeviceIdType.MESH
F32, BF16, I32 = jnp.float32, jnp.bfloat16, jnp.int32

BLOCK = 64
SEG = 256
ROWS = 128
HEADS = 4
PAIRS = HEADS // 2
WIDTH = 2048
CHUNKS = WIDTH // 128
HIDDEN = 512
DEVICES = 128
CAP = 3
SLOTS = DEVICES * CAP


def dot(a, b, dims=((1,), (0,))):
    return lax.dot_general(a, b, (dims, ((), ())), preferred_element_type=F32)


def split3(x):
    high = x.astype(BF16)
    rest = x - high.astype(F32)
    mid = rest.astype(BF16)
    return high, mid, (rest - mid.astype(F32)).astype(BF16)


def iota(shape, dim):
    return lax.broadcasted_iota(I32, shape, dim)


def silu(x):
    return x / (1.0 + jnp.exp(-x))


def kernel(
    residual, queries, keys, values, out_gate, gate_logits, head_gain, out_weight, norm_gain,
    routes, group_score, expert_score, gate_weight, up_weight, down_weight,
    out,
    q_v, k_v, v_v, og_v, gl_v, res_v, ow_v, gw_v, uw_v, dw_v,
    f_v, qd_v, att_v, gain_v, mix_v, pair_v, states, decays, perm_v, pick_v, comb_v,
    merged_v, norm_v, nat_v, send_v, recv_v, inner_v, back_v, ret_v,
    in_sem, w_sem, s_send, s_recv, d_send, d_recv, p_send, p_recv, x_send, x_recv, y_send, y_recv,
):
    place = [lax.axis_index(axis) for axis in AXES]
    core = place[3]
    me = ((place[0] * 4 + place[1]) * 4 + place[2]) * 2 + core

    def shifted(axis, step):
        there = list(place)
        size = 2 if axis == 3 else 4
        there[axis] = (place[axis] + step) % size
        return tuple(there)

    def fetch(pairs, sems, first):
        copies = [
            pltpu.make_async_copy(src, dst, sems.at[first + i]) for i, (src, dst) in enumerate(pairs)
        ]
        for copy in copies:
            copy.start()
        return copies

    get_gl, get_k, get_v, get_q, get_og, get_res = fetch(
        (
            (gate_logits, gl_v), (keys, k_v), (values, v_v), (queries, q_v), (out_gate, og_v),
            (residual, res_v),
        ),
        in_sem,
        0,
    )
    get_ow, get_gw, get_uw, get_dw = fetch(
        (
            (out_weight, ow_v), (gate_weight.at[0], gw_v), (up_weight.at[0], uw_v),
            (down_weight.at[0], dw_v),
        ),
        w_sem,
        0,
    )

    barrier = pltpu.get_barrier_semaphore()
    friends = [(axis, step) for axis in range(3) for step in (1, 2, 3)] + [(3, 1)]
    for axis, step in friends:
        pl.semaphore_signal(
            barrier, inc=1, device_id=shifted(axis, step), device_id_type=MESH
        )

    get_gl.wait()
    x = -gl_v[...].astype(F32)
    decay = -(jnp.maximum(x, 0.0) + jnp.log1p(jnp.exp(-jnp.abs(x)))) * (1.0 / 16.0)
    lower = jnp.where(iota((SEG, SEG), 0) >= iota((SEG, SEG), 1), 1.0, 0.0).astype(BF16)
    high, mid, low = split3(decay)
    f_v[...] = (dot(lower, low) + dot(lower, mid)) + dot(lower, high)

    def end_row(n):
        return f_v[pl.ds(n * BLOCK - 1, 1), :]

    lane_low = iota((1, 128), 1) < 64

    def state_after(n):
        rows = n * BLOCK
        aged = k_v[0:rows, :].astype(F32) * jnp.exp(end_row(n) - f_v[0:rows, :])
        aged = aged.astype(BF16)
        pairs = []
        for p in range(PAIRS):
            side = [
                dot(
                    v_v[0:rows, (2 * p + i) * 128 : (2 * p + i + 1) * 128],
                    aged[:, p * 128 : (p + 1) * 128],
                    ((0,), (0,)),
                )
                for i in range(2)
            ]
            pairs.append(jnp.where(lane_low, side[0], side[1]))
        return pairs

    get_k.wait()
    get_v.wait()
    local_end = state_after(SEG // BLOCK)
    spot = place[2]
    for p in range(PAIRS):
        states[2, spot, :, p * 128 : (p + 1) * 128] = local_end[p].astype(BF16)
    decays[2, spot] = jnp.broadcast_to(end_row(SEG // BLOCK), (8, 256))
    pl.semaphore_wait(barrier, len(friends))

    def share(level):
        here = place[level]
        for step in (2, 1, 3):
            for buf, ss, rs in ((states, s_send, s_recv), (decays, d_send, d_recv)):
                pltpu.make_async_remote_copy(
                    src_ref=buf.at[level, here],
                    dst_ref=buf.at[level, here],
                    send_sem=ss.at[level],
                    recv_sem=rs.at[level],
                    device_id=shifted(level, step),
                    device_id_type=MESH,
                ).start()

    def await_share(level):
        for buf, ss, rs in ((states, s_send, s_recv), (decays, d_send, d_recv)):
            three = buf.at[level, pl.ds(0, 3)]
            pltpu.make_async_copy(three, three, rs.at[level]).wait()
            pltpu.make_async_copy(three, three, ss.at[level]).wait()

    def run_line(level):
        here = place[level]
        state = jnp.zeros((128, 256), F32)
        total = jnp.zeros((1, 256), F32)
        enter, before = state, total
        for j in range(4):
            enter = jnp.where(here == j, state, enter)
            before = jnp.where(here == j, total, before)
            step = decays[level, j, 0:1, :]
            state = state * jnp.exp(step) + states[level, j].astype(F32)
            total = total + step
        return enter, before, state, total

    share(2)

    get_q.wait()
    scale = 64.0 ** (-0.5)
    block_row = iota((SEG, 1), 0) // BLOCK
    f = f_v[...]
    start = jnp.zeros((SEG, 256), F32)
    for n in range(1, SEG // BLOCK):
        start = jnp.where(block_row == n, end_row(n), start)
    running = f - start
    q = q_v[...].astype(F32) * scale
    qd_v[...] = (q * jnp.exp(f)).astype(BF16)
    q_scaled = (q * jnp.exp(running)).astype(BF16)
    k_inverse = (k_v[...].astype(F32) * jnp.exp(-running)).astype(BF16)
    row, col = iota((SEG, SEG), 0), iota((SEG, SEG), 1)
    causal = (row >= col) & (row // BLOCK == col // BLOCK)
    none = jnp.zeros((), BF16)
    local_states = [None] + [
        [s.astype(BF16) for s in state_after(n)] for n in range(1, SEG // BLOCK)
    ]
    for h in range(HEADS):
        p = h // 2
        mine = lane_low if h % 2 == 0 else jnp.logical_not(lane_low)
        lanes = slice(p * 128, (p + 1) * 128)
        q_h = jnp.where(mine, q_scaled[:, lanes], none)
        k_h = jnp.where(mine, k_inverse[:, lanes], none)
        scores = jnp.where(causal, dot(q_h, k_h, ((1,), (1,))), 0.0).astype(BF16)
        here = slice(h * 128, (h + 1) * 128)
        att_v[:, here] = dot(scores, v_v[:, here])
        for n in range(1, SEG // BLOCK):
            rows = slice(n * BLOCK, (n + 1) * BLOCK)
            att_v[rows, here] += dot(q_h[rows], local_states[n][p], ((1,), (1,)))
    get_og.wait()
    for h in range(HEADS):
        here = slice(h * 128, (h + 1) * 128)
        gain_v[:, here] = silu(og_v[:, here].astype(F32)) * head_gain[...]

    diagonal = iota((128, 128), 0) == iota((128, 128), 1)

    def as_row(column):
        return jnp.sum(jnp.where(diagonal, column, 0.0), axis=0, keepdims=True)

    def as_column(line):
        return jnp.sum(jnp.where(diagonal, line, 0.0), axis=1, keepdims=True)

    expert_id = iota((128, 128), 0).astype(F32)
    earlier = jnp.where(iota((128, 128), 0) < iota((128, 128), 1), 1.0, 0.0).astype(BF16)
    taken = jnp.zeros((128, 1), F32)
    slot_rows = []
    for c in range(2):
        line = as_row(routes[:, c : c + 1].astype(F32))
        hit = jnp.where(expert_id == line, 1.0, 0.0)
        count = dot(hit.astype(BF16), earlier) + taken
        rank = jnp.sum(hit * count, axis=0, keepdims=True)
        slot_rows.append(line * CAP + rank)
        taken = taken + jnp.sum(hit, axis=1, keepdims=True)
    slot_id = iota((SLOTS, 128), 0).astype(F32)
    pick_v[...] = (
        jnp.where(slot_id == slot_rows[0], 1.0, 0.0) + jnp.where(slot_id == slot_rows[1], 1.0, 0.0)
    ).astype(BF16)
    score = expert_score[...]
    score_sum = score[:, 0:1] + score[:, 1:2]
    group = as_column(group_score[...])
    slot_lane = iota((ROWS, SLOTS), 1).astype(F32)
    comb = jnp.zeros((ROWS, SLOTS), F32)
    for c in range(2):
        weight = group * score[:, c : c + 1] / score_sum
        comb = comb + jnp.where(slot_lane == as_column(slot_rows[c]), weight, 0.0)
    for i, part in enumerate(split3(comb)[:2]):
        comb_v[i] = part
    row, col = iota((256, 256), 0), iota((256, 256), 1)
    perm_v[...] = jnp.where(row == (col % 16) * 16 + col // 16, 1.0, 0.0).astype(BF16)

    entering = None
    scales = []
    enters = []
    for level in (2, 1, 0):
        await_share(level)
        enter, before, state, total = run_line(level)
        if level:
            upper = level - 1
            states[upper, place[upper]] = state.astype(BF16)
            decays[upper, place[upper]] = jnp.broadcast_to(total, (8, 256))
            share(upper)
        enters.append(enter)
        scales.append(jnp.exp(before))
    entering = enters[0] + scales[0] * (enters[1] + scales[1] * enters[2])
    entering = entering.astype(BF16)

    for h in range(HEADS):
        p = h // 2
        mine = lane_low if h % 2 == 0 else jnp.logical_not(lane_low)
        lanes = slice(p * 128, (p + 1) * 128)
        here = slice(h * 128, (h + 1) * 128)
        q_h = jnp.where(mine, qd_v[:, lanes], none)
        attended = att_v[:, here] + dot(q_h, entering[:, lanes], ((1,), (1,)))
        mean = jnp.mean(attended * attended, axis=-1, keepdims=True)
        mix_v[:, here] = (attended * lax.rsqrt(mean + 1e-06) * gain_v[:, here]).astype(BF16)
    other_rows = pl.ds(pl.multiple_of((1 - core) * ROWS, ROWS), ROWS)
    own_rows = pl.ds(pl.multiple_of(core * ROWS, ROWS), ROWS)
    swap = pltpu.make_async_remote_copy(
        src_ref=mix_v.at[other_rows],
        dst_ref=pair_v,
        send_sem=p_send,
        recv_sem=p_recv,
        device_id=shifted(3, 1),
        device_id_type=MESH,
    )
    swap.start()
    get_res.wait()
    get_ow.wait()
    half = HEADS * 128
    own_w = pl.ds(pl.multiple_of(core * half, half), half)
    other_w = pl.ds(pl.multiple_of((1 - core) * half, half), half)
    summed = res_v[...].astype(F32) + dot(mix_v[own_rows, :], ow_v[own_w, :])
    swap.wait()
    summed = summed + dot(pair_v[...], ow_v[other_w, :])
    merged = summed.astype(BF16)
    merged_v[...] = merged
    wide = merged.astype(F32)
    mean = jnp.mean(wide * wide, axis=-1, keepdims=True)
    norm_v[...] = (wide * lax.rsqrt(mean + 1e-06) * norm_gain[...]).astype(BF16)

    nat_v[...] = dot(pick_v[...], norm_v[...]).astype(BF16)

    def to_tiles(src, dst):
        @pl.loop(0, SLOTS // 16)
        def _(g):
            rows = pl.ds(pl.multiple_of(g * 16, 16), 16)
            stack = jnp.concatenate(
                [src[rows, j * 128 : (j + 1) * 128] for j in range(CHUNKS)], axis=0
            )
            moved = dot(perm_v[...], stack).astype(BF16)
            dst[rows] = moved.reshape(16, CHUNKS, 128)

    def from_tiles(src, dst):
        @pl.loop(0, SLOTS // 16)
        def _(g):
            rows = pl.ds(pl.multiple_of(g * 16, 16), 16)
            moved = dot(perm_v[...], src[rows].reshape(16 * CHUNKS, 128)).astype(BF16)
            for j in range(CHUNKS):
                dst[rows, j * 128 : (j + 1) * 128] = moved[j * 16 : (j + 1) * 16]

    def exchange(src, dst, ss, rs):
        @pl.loop(1, DEVICES)
        def _(i):
            offset = (i * 53) % DEVICES
            steps = (offset // 32, (offset // 8) % 4, (offset // 2) % 4, offset % 2)
            there = tuple(
                (place[a] + steps[a]) % (2 if a == 3 else 4) for a in range(4)
            )
            peer = ((there[0] * 4 + there[1]) * 4 + there[2]) * 2 + there[3]
            pltpu.make_async_remote_copy(
                src_ref=src.at[pl.ds(peer * CAP, CAP)],
                dst_ref=dst.at[pl.ds(me * CAP, CAP)],
                send_sem=ss,
                recv_sem=rs,
                device_id=there,
                device_id_type=MESH,
            ).start()

        mine = pl.ds(me * CAP, CAP)
        dst[mine] = src[mine]

    def await_exchange(src, dst, ss, rs):
        most = pl.ds(0, (DEVICES - 1) * CAP)
        pltpu.make_async_copy(src.at[most], dst.at[most], rs).wait()
        pltpu.make_async_copy(src.at[most], dst.at[most], ss).wait()

    to_tiles(nat_v, send_v)
    exchange(send_v, recv_v, x_send, x_recv)
    get_gw.wait()
    get_uw.wait()
    get_dw.wait()
    await_exchange(send_v, recv_v, x_send, x_recv)
    from_tiles(recv_v, nat_v)

    @pl.loop(0, HIDDEN // 256)
    def _(n):
        cols = pl.ds(pl.multiple_of(n * 256, 256), 256)
        gated = dot(nat_v[...], gw_v[:, cols])
        lifted = dot(nat_v[...], uw_v[:, cols])
        inner_v[:, cols] = (silu(gated) * lifted).astype(BF16)

    @pl.loop(0, WIDTH // 256)
    def _(n):
        cols = pl.ds(pl.multiple_of(n * 256, 256), 256)
        nat_v[:, cols] = dot(inner_v[...], dw_v[:, cols]).astype(BF16)

    to_tiles(nat_v, back_v)
    exchange(back_v, ret_v, y_send, y_recv)
    await_exchange(back_v, ret_v, y_send, y_recv)
    from_tiles(ret_v, nat_v)

    @pl.loop(0, WIDTH // 256)
    def _(n):
        cols = pl.ds(pl.multiple_of(n * 256, 256), 256)
        combined = dot(comb_v[1], nat_v[:, cols]) + dot(comb_v[0], nat_v[:, cols])
        out[:, cols] = (merged_v[:, cols].astype(F32) + combined).astype(BF16)


def local(
    residual, queries, key_rows, value_rows, out_gate, gate_logits, head_gain, out_weight,
    norm_gain, routes, group_score, expert_score, gate_weight, up_weight, down_weight,
):
    anywhere = pl.BlockSpec(memory_space=pl.ANY)
    vmem = pl.BlockSpec(memory_space=pltpu.VMEM)
    half = HEADS * 128
    tiles = pltpu.VMEM((SLOTS, CHUNKS, 128), BF16)
    dma = pltpu.SemaphoreType.DMA
    return pl.pallas_call(
        kernel,
        out_shape=jax.ShapeDtypeStruct((ROWS, WIDTH), BF16),
        in_specs=[anywhere] * 6 + [vmem, anywhere, vmem, vmem, vmem, vmem] + [anywhere] * 3,
        out_specs=vmem,
        scratch_shapes=[
            pltpu.VMEM((SEG, 256), BF16),
            pltpu.VMEM((SEG, 256), BF16),
            pltpu.VMEM((SEG, half), BF16),
            pltpu.VMEM((SEG, half), BF16),
            pltpu.VMEM((SEG, 256), BF16),
            pltpu.VMEM((ROWS, WIDTH), BF16),
            pltpu.VMEM((2 * half, WIDTH), BF16),
            pltpu.VMEM((WIDTH, HIDDEN), BF16),
            pltpu.VMEM((WIDTH, HIDDEN), BF16),
            pltpu.VMEM((HIDDEN, WIDTH), BF16),
            pltpu.VMEM((SEG, 256), F32),
            pltpu.VMEM((SEG, 256), BF16),
            pltpu.VMEM((SEG, half), F32),
            pltpu.VMEM((SEG, half), F32),
            pltpu.VMEM((SEG, half), BF16),
            pltpu.VMEM((ROWS, half), BF16),
            pltpu.VMEM((3, 4, 128, 256), BF16),
            pltpu.VMEM((3, 4, 8, 256), F32),
            pltpu.VMEM((256, 256), BF16),
            pltpu.VMEM((SLOTS, ROWS), BF16),
            pltpu.VMEM((2, ROWS, SLOTS), BF16),
            pltpu.VMEM((ROWS, WIDTH), BF16),
            pltpu.VMEM((ROWS, WIDTH), BF16),
            pltpu.VMEM((SLOTS, WIDTH), BF16),
            tiles,
            tiles,
            pltpu.VMEM((SLOTS, HIDDEN), BF16),
            tiles,
            tiles,
            dma((6,)), dma((4,)),
            dma((3,)), dma((3,)), dma((3,)), dma((3,)),
            dma, dma, dma, dma, dma, dma,
        ],
        compiler_params=pltpu.CompilerParams(
            collective_id=0, has_side_effects=True, vmem_limit_bytes=56 * 2**20
        ),
    )(
        residual, queries, key_rows, value_rows, out_gate, gate_logits,
        head_gain.reshape(1, 128), out_weight, norm_gain.reshape(1, WIDTH),
        routes, group_score.reshape(1, ROWS), expert_score, gate_weight, up_weight, down_weight,
    )


def solution(mesh):
    torus = Mesh(mesh.devices.reshape(4, 4, 4, mesh.shape["tp"]), AXES)
    both = P(AXES)
    in_specs = (
        P(AXES, None),
        P(SP, "tp"), P(SP, "tp"), P(SP, "tp"), P(SP, "tp"), P(SP, "tp"),
        P(), P(), P(),
        P(AXES, None), both, P(AXES, None),
        P(AXES, None, None), P(AXES, None, None), P(AXES, None, None),
    )
    return jax.shard_map(
        local, mesh=torus, in_specs=in_specs, out_specs=P(AXES, None), check_vma=False
    )
```

```python
import jax
import jax.numpy as jnp
from jax import lax
from jax.experimental import pallas as pl
from jax.experimental.pallas import tpu as pltpu
from jax.sharding import Mesh
from jax.sharding import PartitionSpec as P

AXES = ("sp_0", "sp_1", "sp_2", "tp")
SP = AXES[:3]
MESH = pl.DeviceIdType.MESH
F32, BF16, I32 = jnp.float32, jnp.bfloat16, jnp.int32

BLOCK = 64
SEG = 256
ROWS = 128
HEADS = 4
PAIRS = HEADS // 2
WIDTH = 2048
CHUNKS = WIDTH // 128
HIDDEN = 512
DEVICES = 128
CAP = 3
SLOTS = DEVICES * CAP
PARTS = 4
STEPS = DEVICES // PARTS
PART = STEPS * CAP
STRIDE, UNSTRIDE = 53, 29
PITCH = CHUNKS + 1


def dot(a, b, dims=((1,), (0,))):
    return lax.dot_general(a, b, (dims, ((), ())), preferred_element_type=F32)


def split3(x):
    high = x.astype(BF16)
    rest = x - high.astype(F32)
    mid = rest.astype(BF16)
    return high, mid, (rest - mid.astype(F32)).astype(BF16)


def iota(shape, dim):
    return lax.broadcasted_iota(I32, shape, dim)


def silu(x):
    return x / (1.0 + jnp.exp(-x))


def kernel(
    residual, queries, keys, values, out_gate, gate_logits, head_gain, out_weight, norm_gain,
    routes, group_score, expert_score, gate_weight, up_weight, down_weight,
    out,
    q_v, k_v, v_v, og_v, gl_v, res_v, ow_v, gw_v, uw_v, dw_v,
    f_v, qd_v, att_v, gain_v, mix_v, pair_v, states, decays, pick_v, comb_v,
    norm_v, acc_v, nat_v, tile_v, send_v, recv_v, inner_v, back_v, ret_v,
    in_sem, w_sem, s_send, s_recv, d_send, d_recv, p_send, p_recv, x_send, x_recv, y_send, y_recv,
):
    place = [lax.axis_index(axis) for axis in AXES]
    core = place[3]
    me = ((place[0] * 4 + place[1]) * 4 + place[2]) * 2 + core

    def shifted(axis, step):
        there = list(place)
        size = 2 if axis == 3 else 4
        there[axis] = (place[axis] + step) % size
        return tuple(there)

    def fetch(pairs, sems, first):
        copies = [
            pltpu.make_async_copy(src, dst, sems.at[first + i]) for i, (src, dst) in enumerate(pairs)
        ]
        for copy in copies:
            copy.start()
        return copies

    get_gl, get_k, get_v, get_q, get_og, get_res = fetch(
        (
            (gate_logits, gl_v), (keys, k_v), (values, v_v), (queries, q_v), (out_gate, og_v),
            (residual, res_v),
        ),
        in_sem,
        0,
    )
    get_ow, get_gw, get_uw, get_dw = fetch(
        (
            (out_weight, ow_v), (gate_weight.at[0], gw_v), (up_weight.at[0], uw_v),
            (down_weight.at[0], dw_v),
        ),
        w_sem,
        0,
    )

    barrier = pltpu.get_barrier_semaphore()
    friends = [(axis, step) for axis in range(3) for step in (1, 2, 3)] + [(3, 1)]
    for axis, step in friends:
        pl.semaphore_signal(
            barrier, inc=1, device_id=shifted(axis, step), device_id_type=MESH
        )

    get_gl.wait()
    x = -gl_v[...].astype(F32)
    decay = -(jnp.maximum(x, 0.0) + jnp.log1p(jnp.exp(-jnp.abs(x)))) * (1.0 / 16.0)
    lower = jnp.where(iota((SEG, SEG), 0) >= iota((SEG, SEG), 1), 1.0, 0.0).astype(BF16)
    high, mid, low = split3(decay)
    f_v[...] = (dot(lower, low) + dot(lower, mid)) + dot(lower, high)

    def end_row(n):
        return f_v[pl.ds(n * BLOCK - 1, 1), :]

    lane_low = iota((1, 128), 1) < 64

    def state_after(n):
        rows = n * BLOCK
        aged = k_v[0:rows, :].astype(F32) * jnp.exp(end_row(n) - f_v[0:rows, :])
        aged = aged.astype(BF16)
        pairs = []
        for p in range(PAIRS):
            side = [
                dot(
                    v_v[0:rows, (2 * p + i) * 128 : (2 * p + i + 1) * 128],
                    aged[:, p * 128 : (p + 1) * 128],
                    ((0,), (0,)),
                )
                for i in range(2)
            ]
            pairs.append(jnp.where(lane_low, side[0], side[1]))
        return pairs

    get_k.wait()
    get_v.wait()
    local_end = state_after(SEG // BLOCK)
    spot = place[2]
    for p in range(PAIRS):
        states[2, spot, :, p * 128 : (p + 1) * 128] = local_end[p].astype(BF16)
    decays[2, spot] = jnp.broadcast_to(end_row(SEG // BLOCK), (8, 256))
    pl.semaphore_wait(barrier, len(friends))

    def share(level):
        here = place[level]
        for step in (2, 1, 3):
            for buf, ss, rs in ((states, s_send, s_recv), (decays, d_send, d_recv)):
                pltpu.make_async_remote_copy(
                    src_ref=buf.at[level, here],
                    dst_ref=buf.at[level, here],
                    send_sem=ss.at[level],
                    recv_sem=rs.at[level],
                    device_id=shifted(level, step),
                    device_id_type=MESH,
                ).start()

    def await_share(level):
        for buf, ss, rs in ((states, s_send, s_recv), (decays, d_send, d_recv)):
            three = buf.at[level, pl.ds(0, 3)]
            pltpu.make_async_copy(three, three, rs.at[level]).wait()
            pltpu.make_async_copy(three, three, ss.at[level]).wait()

    def run_line(level):
        here = place[level]
        state = jnp.zeros((128, 256), F32)
        total = jnp.zeros((1, 256), F32)
        enter, before = state, total
        for j in range(4):
            enter = jnp.where(here == j, state, enter)
            before = jnp.where(here == j, total, before)
            step = decays[level, j, 0:1, :]
            state = state * jnp.exp(step) + states[level, j].astype(F32)
            total = total + step
        return enter, before, state, total

    share(2)

    get_q.wait()
    scale = 64.0 ** (-0.5)
    block_row = iota((SEG, 1), 0) // BLOCK
    f = f_v[...]
    start = jnp.zeros((SEG, 256), F32)
    for n in range(1, SEG // BLOCK):
        start = jnp.where(block_row == n, end_row(n), start)
    running = f - start
    q = q_v[...].astype(F32) * scale
    qd_v[...] = (q * jnp.exp(f)).astype(BF16)
    q_scaled = (q * jnp.exp(running)).astype(BF16)
    k_inverse = (k_v[...].astype(F32) * jnp.exp(-running)).astype(BF16)
    row, col = iota((SEG, SEG), 0), iota((SEG, SEG), 1)
    causal = (row >= col) & (row // BLOCK == col // BLOCK)
    none = jnp.zeros((), BF16)
    local_states = [None] + [
        [s.astype(BF16) for s in state_after(n)] for n in range(1, SEG // BLOCK)
    ]
    for h in range(HEADS):
        p = h // 2
        mine = lane_low if h % 2 == 0 else jnp.logical_not(lane_low)
        lanes = slice(p * 128, (p + 1) * 128)
        q_h = jnp.where(mine, q_scaled[:, lanes], none)
        k_h = jnp.where(mine, k_inverse[:, lanes], none)
        scores = jnp.where(causal, dot(q_h, k_h, ((1,), (1,))), 0.0).astype(BF16)
        here = slice(h * 128, (h + 1) * 128)
        att_v[:, here] = dot(scores, v_v[:, here])
        for n in range(1, SEG // BLOCK):
            rows = slice(n * BLOCK, (n + 1) * BLOCK)
            att_v[rows, here] += dot(q_h[rows], local_states[n][p], ((1,), (1,)))
    get_og.wait()
    for h in range(HEADS):
        here = slice(h * 128, (h + 1) * 128)
        gain_v[:, here] = silu(og_v[:, here].astype(F32)) * head_gain[...]

    diagonal = iota((128, 128), 0) == iota((128, 128), 1)

    def as_column(line):
        return jnp.sum(jnp.where(diagonal, line, 0.0), axis=1, keepdims=True)

    expert_id = iota((128, 128), 0)
    earlier = jnp.where(iota((128, 128), 0) < iota((128, 128), 1), 1.0, 0.0).astype(BF16)
    taken = jnp.zeros((128, 1), F32)
    slot_rows = []
    for c in range(2):
        line = routes[c : c + 1, :]
        hit = jnp.where(expert_id == line, 1.0, 0.0)
        count = dot(hit.astype(BF16), earlier) + taken
        rank = jnp.sum(hit * count, axis=0, keepdims=True)
        offset = jnp.zeros_like(line)
        for a, unit in enumerate((32, 8, 2, 1)):
            size = 2 if a == 3 else 4
            offset = offset + unit * ((line // unit % size - place[a] + size) % size)
        step = offset * UNSTRIDE % DEVICES
        slot_rows.append((step * CAP).astype(F32) + rank)
        taken = taken + jnp.sum(hit, axis=1, keepdims=True)
    slot_id = iota((SLOTS, 128), 0).astype(F32)
    pick_v[...] = (
        jnp.where(slot_id == slot_rows[0], 1.0, 0.0) + jnp.where(slot_id == slot_rows[1], 1.0, 0.0)
    ).astype(BF16)
    score = [as_column(expert_score[c : c + 1, :]) for c in range(2)]
    group = as_column(group_score[...])
    slot_columns = [as_column(line) for line in slot_rows]
    for part in range(PARTS):
        slot_lane = (iota((ROWS, PART), 1) + part * PART).astype(F32)
        comb = jnp.zeros((ROWS, PART), F32)
        for c in range(2):
            weight = group * score[c] / (score[0] + score[1])
            comb = comb + jnp.where(slot_lane == slot_columns[c], weight, 0.0)
        high, mid, _ = split3(comb)
        comb_v[part, 0:ROWS] = mid
        comb_v[part, ROWS : 2 * ROWS] = high

    entering = None
    scales = []
    enters = []
    for level in (2, 1, 0):
        await_share(level)
        enter, before, state, total = run_line(level)
        if level:
            upper = level - 1
            states[upper, place[upper]] = state.astype(BF16)
            decays[upper, place[upper]] = jnp.broadcast_to(total, (8, 256))
            share(upper)
        enters.append(enter)
        scales.append(jnp.exp(before))
    entering = enters[0] + scales[0] * (enters[1] + scales[1] * enters[2])
    entering = entering.astype(BF16)

    for h in range(HEADS):
        p = h // 2
        mine = lane_low if h % 2 == 0 else jnp.logical_not(lane_low)
        lanes = slice(p * 128, (p + 1) * 128)
        here = slice(h * 128, (h + 1) * 128)
        q_h = jnp.where(mine, qd_v[:, lanes], none)
        attended = att_v[:, here] + dot(q_h, entering[:, lanes], ((1,), (1,)))
        mean = jnp.mean(attended * attended, axis=-1, keepdims=True)
        mix_v[:, here] = (attended * lax.rsqrt(mean + 1e-06) * gain_v[:, here]).astype(BF16)
    other_rows = pl.ds(pl.multiple_of((1 - core) * ROWS, ROWS), ROWS)
    own_rows = pl.ds(pl.multiple_of(core * ROWS, ROWS), ROWS)
    swap = pltpu.make_async_remote_copy(
        src_ref=mix_v.at[other_rows],
        dst_ref=pair_v,
        send_sem=p_send,
        recv_sem=p_recv,
        device_id=shifted(3, 1),
        device_id_type=MESH,
    )
    swap.start()
    get_res.wait()
    get_ow.wait()
    half = HEADS * 128
    own_w = pl.ds(pl.multiple_of(core * half, half), half)
    other_w = pl.ds(pl.multiple_of((1 - core) * half, half), half)
    summed = res_v[...].astype(F32) + dot(mix_v[own_rows, :], ow_v[own_w, :])
    swap.wait()
    summed = summed + dot(pair_v[...], ow_v[other_w, :])
    wide = summed.astype(BF16).astype(F32)
    acc_v[...] = wide
    mean = jnp.mean(wide * wide, axis=-1, keepdims=True)
    norm_v[...] = (wide * lax.rsqrt(mean + 1e-06) * norm_gain[...]).astype(BF16)

    def put_columns(j, block):
        for i in range(2):
            tile_v[pl.ds(2 * j + i, PART, stride=PITCH), :] = block[:, i * 128 : (i + 1) * 128]

    def gather_tiles(dst, part):
        @pl.loop(0, PART // 16)
        def _(g):
            for i in range(16):
                slot = g * 16 + i
                dst[part * PART + slot] = tile_v[pl.ds(slot * PITCH, CHUNKS), :].astype(BF16)

    def to_rows(src, part):
        @pl.loop(0, PART // 32)
        def _(g):
            for i in range(2):
                rows = pl.ds(pl.multiple_of(g * 32 + i * 16, 16), 16)
                nat_v[rows, :] = src[pl.ds(part * PART + g * 32 + i * 16, 16)].reshape(16, WIDTH)

    def send_part(part, src, dst, ss, rs, sign):
        @pl.loop(max(1, part * STEPS), (part + 1) * STEPS)
        def _(i):
            offset = lax.rem(i * STRIDE, DEVICES)
            steps = (
                lax.div(offset, 32), lax.rem(lax.div(offset, 8), 4), lax.rem(lax.div(offset, 2), 4),
                lax.rem(offset, 2),
            )
            there = tuple(
                lax.rem(place[a] + sign * steps[a] + 4, 2 if a == 3 else 4) for a in range(4)
            )
            rows = pl.ds(i * CAP, CAP)
            pltpu.make_async_remote_copy(
                src_ref=src.at[rows],
                dst_ref=dst.at[rows],
                send_sem=ss,
                recv_sem=rs.at[part],
                device_id=there,
                device_id_type=MESH,
            ).start()

        if part == 0:
            dst[0:CAP] = src[0:CAP]

    def await_part(part, dst, rs):
        count = PART - (CAP if part == 0 else 0)
        rows = dst.at[pl.ds(part * PART, count)]
        pltpu.make_async_copy(rows, rows, rs.at[part]).wait()

    for part in range(PARTS):
        chosen = pick_v[part * PART : (part + 1) * PART, :]
        for j in range(WIDTH // 256):
            put_columns(j, dot(chosen, norm_v[:, j * 256 : (j + 1) * 256]))
        gather_tiles(send_v, part)
        send_part(part, send_v, recv_v, x_send, x_recv, 1)
    get_gw.wait()
    get_uw.wait()
    get_dw.wait()
    for part in range(PARTS):
        await_part(part, recv_v, x_recv)
        to_rows(recv_v, part)
        for n in range(HIDDEN // 256):
            cols = slice(n * 256, (n + 1) * 256)
            gated = dot(nat_v[...], gw_v[:, cols])
            lifted = dot(nat_v[...], uw_v[:, cols])
            inner_v[:, cols] = (silu(gated) * lifted).astype(BF16)
        for j in range(WIDTH // 256):
            put_columns(j, dot(inner_v[...], dw_v[:, j * 256 : (j + 1) * 256]))
        gather_tiles(back_v, part)
        send_part(part, back_v, ret_v, y_send, y_recv, -1)
    for part in range(PARTS):
        await_part(part, ret_v, y_recv)
        to_rows(ret_v, part)
        for j in range(WIDTH // 256):
            cols = slice(j * 256, (j + 1) * 256)
            both = dot(comb_v[part], nat_v[:, cols])
            total = acc_v[:, cols] + (both[0:ROWS] + both[ROWS : 2 * ROWS])
            if part < PARTS - 1:
                acc_v[:, cols] = total
            else:
                out[:, cols] = total.astype(BF16)
    for src, ss in ((send_v, x_send), (back_v, y_send)):
        rows = src.at[pl.ds(0, SLOTS - CAP)]
        pltpu.make_async_copy(rows, rows, ss).wait()


def local(
    residual, queries, key_rows, value_rows, out_gate, gate_logits, head_gain, out_weight,
    norm_gain, routes, group_score, expert_score, gate_weight, up_weight, down_weight,
):
    anywhere = pl.BlockSpec(memory_space=pl.ANY)
    vmem = pl.BlockSpec(memory_space=pltpu.VMEM)
    half = HEADS * 128
    tiles = pltpu.VMEM((SLOTS, CHUNKS, 128), BF16)
    dma = pltpu.SemaphoreType.DMA
    return pl.pallas_call(
        kernel,
        out_shape=jax.ShapeDtypeStruct((ROWS, WIDTH), BF16),
        in_specs=[anywhere] * 6 + [vmem, anywhere, vmem, vmem, vmem, vmem] + [anywhere] * 3,
        out_specs=vmem,
        scratch_shapes=[
            pltpu.VMEM((SEG, 256), BF16),
            pltpu.VMEM((SEG, 256), BF16),
            pltpu.VMEM((SEG, half), BF16),
            pltpu.VMEM((SEG, half), BF16),
            pltpu.VMEM((SEG, 256), BF16),
            pltpu.VMEM((ROWS, WIDTH), BF16),
            pltpu.VMEM((2 * half, WIDTH), BF16),
            pltpu.VMEM((WIDTH, HIDDEN), BF16),
            pltpu.VMEM((WIDTH, HIDDEN), BF16),
            pltpu.VMEM((HIDDEN, WIDTH), BF16),
            pltpu.VMEM((SEG, 256), F32),
            pltpu.VMEM((SEG, 256), BF16),
            pltpu.VMEM((SEG, half), F32),
            pltpu.VMEM((SEG, half), F32),
            pltpu.VMEM((SEG, half), BF16),
            pltpu.VMEM((ROWS, half), BF16),
            pltpu.VMEM((3, 4, 128, 256), BF16),
            pltpu.VMEM((3, 4, 8, 256), F32),
            pltpu.VMEM((SLOTS, ROWS), BF16),
            pltpu.VMEM((PARTS, 2 * ROWS, PART), BF16),
            pltpu.VMEM((ROWS, WIDTH), BF16),
            pltpu.VMEM((ROWS, WIDTH), F32),
            pltpu.VMEM((PART, WIDTH), BF16),
            pltpu.VMEM((PART * PITCH, 128), F32),
            tiles,
            tiles,
            pltpu.VMEM((PART, HIDDEN), BF16),
            tiles,
            tiles,
            dma((6,)), dma((4,)),
            dma((3,)), dma((3,)), dma((3,)), dma((3,)),
            dma, dma, dma, dma((PARTS,)), dma, dma((PARTS,)),
        ],
        compiler_params=pltpu.CompilerParams(
            collective_id=0, has_side_effects=True, vmem_limit_bytes=56 * 2**20
        ),
    )(
        residual, queries, key_rows, value_rows, out_gate, gate_logits,
        head_gain.reshape(1, 128), out_weight, norm_gain.reshape(1, WIDTH),
        routes.T, group_score.reshape(1, ROWS), expert_score.T, gate_weight, up_weight, down_weight,
    )


def solution(mesh):
    torus = Mesh(mesh.devices.reshape(4, 4, 4, mesh.shape["tp"]), AXES)
    both = P(AXES)
    in_specs = (
        P(AXES, None),
        P(SP, "tp"), P(SP, "tp"), P(SP, "tp"), P(SP, "tp"), P(SP, "tp"),
        P(), P(), P(),
        P(AXES, None), both, P(AXES, None),
        P(AXES, None, None), P(AXES, None, None), P(AXES, None, None),
    )
    return jax.shard_map(
        local, mesh=torus, in_specs=in_specs, out_specs=P(AXES, None), check_vma=False
    )
```

```python
import jax
import jax.numpy as jnp
from jax import lax
from jax.experimental import pallas as pl
from jax.experimental.pallas import tpu as pltpu
from jax.sharding import Mesh
from jax.sharding import PartitionSpec as P

AXES = ("sp_0", "sp_1", "sp_2", "tp")
SP = AXES[:3]
MESH = pl.DeviceIdType.MESH
F32, BF16, I32 = jnp.float32, jnp.bfloat16, jnp.int32

BLOCK = 64
SEG = 256
ROWS = 128
HEADS = 4
PAIRS = HEADS // 2
WIDTH = 2048
CHUNKS = WIDTH // 128
HIDDEN = 512
DEVICES = 128
CAP = 3
SLOTS = DEVICES * CAP
PARTS = 4
STEPS = DEVICES // PARTS
PART = STEPS * CAP
STRIDE, UNSTRIDE = 53, 29
PITCH = CHUNKS + 1


def dot(a, b, dims=((1,), (0,))):
    return lax.dot_general(a, b, (dims, ((), ())), preferred_element_type=F32)


def split3(x):
    high = x.astype(BF16)
    rest = x - high.astype(F32)
    mid = rest.astype(BF16)
    return high, mid, (rest - mid.astype(F32)).astype(BF16)


def iota(shape, dim):
    return lax.broadcasted_iota(I32, shape, dim)


def silu(x):
    return x / (1.0 + jnp.exp(-x))


def kernel(
    residual, queries, keys, values, out_gate, gate_logits, head_gain_h, out_weight, norm_gain_h,
    routes_h, group_score_h, expert_score_h, gate_weight, up_weight, down_weight,
    out,
    head_gain, norm_gain, routes, group_score, expert_score,
    q_v, k_v, v_v, og_v, gl_v, res_v, ow_v, gw_v, uw_v, dw_v,
    f_v, qd_v, att_v, gain_v, mix_v, pair_v, states, pick_v, comb_v,
    norm_v, acc_v, nat_v, tile_v, send_v, recv_v, inner_v, back_v, ret_v,
    in_sem, w_sem, s_send, s_recv, p_send, p_recv, x_send, x_recv, y_send, y_recv,
):
    place = [lax.axis_index(axis) for axis in AXES]
    core = place[3]
    me = ((place[0] * 4 + place[1]) * 4 + place[2]) * 2 + core

    def shifted(axis, step):
        there = list(place)
        size = 2 if axis == 3 else 4
        there[axis] = (place[axis] + step) % size
        return tuple(there)

    def fetch(pairs, sems, first):
        copies = [
            pltpu.make_async_copy(src, dst, sems.at[first + i]) for i, (src, dst) in enumerate(pairs)
        ]
        for copy in copies:
            copy.start()
        return copies

    get_gl, get_k, get_v, get_q, get_og, get_res = fetch(
        (
            (gate_logits, gl_v), (keys, k_v), (values, v_v), (queries, q_v), (out_gate, og_v),
            (residual, res_v),
        ),
        in_sem,
        0,
    )
    get_small = fetch(
        (
            (head_gain_h, head_gain), (norm_gain_h, norm_gain), (routes_h, routes),
            (group_score_h, group_score), (expert_score_h, expert_score),
        ),
        in_sem,
        6,
    )
    get_ow, get_gw, get_uw, get_dw = fetch(
        (
            (out_weight, ow_v), (gate_weight.at[0], gw_v), (up_weight.at[0], uw_v),
            (down_weight.at[0], dw_v),
        ),
        w_sem,
        0,
    )

    barrier = pltpu.get_barrier_semaphore()
    friends = [(axis, step) for axis in range(3) for step in (1, 2, 3)] + [(3, 1)]
    for axis, step in friends:
        pl.semaphore_signal(
            barrier, inc=1, device_id=shifted(axis, step), device_id_type=MESH
        )

    get_gl.wait()
    x = -gl_v[...].astype(F32)
    decay = -(jnp.maximum(x, 0.0) + jnp.log1p(jnp.exp(-jnp.abs(x)))) * (1.0 / 16.0)
    lower = jnp.where(iota((SEG, SEG), 0) >= iota((SEG, SEG), 1), 1.0, 0.0).astype(BF16)
    high, mid, low = split3(decay)
    f_v[...] = (dot(lower, low) + dot(lower, mid)) + dot(lower, high)

    def end_row(n):
        return f_v[pl.ds(n * BLOCK - 1, 1), :]

    lane_low = iota((1, 128), 1) < 64

    def state_after(n, p):
        rows, lanes = n * BLOCK, slice(p * 128, (p + 1) * 128)
        aged = k_v[0:rows, lanes].astype(F32) * jnp.exp(end_row(n)[:, lanes] - f_v[0:rows, lanes])
        aged = aged.astype(BF16)
        side = [
            dot(v_v[0:rows, (2 * p + i) * 128 : (2 * p + i + 1) * 128], aged, ((0,), (0,)))
            for i in range(2)
        ]
        return jnp.where(lane_low, side[0], side[1])

    def put_decays(level, p, line):
        part_row = iota((16, 128), 0)
        rows = jnp.zeros((16, 128), F32)
        for i, part in enumerate(split3(line)):
            rows = jnp.where(part_row == i, part.astype(F32), rows)
        states[level, 2 * p, place[level], 64:80, :] = rows.astype(BF16)

    def share(level, piece):
        here = place[level]
        rows = pl.ds(0, 80 if piece % 2 == 0 else 64)
        for step in (2, 1, 3):
            pltpu.make_async_remote_copy(
                src_ref=states.at[level, piece, here, rows],
                dst_ref=states.at[level, piece, here, rows],
                send_sem=s_send.at[level, piece],
                recv_sem=s_recv.at[level, piece],
                device_id=shifted(level, step),
                device_id_type=MESH,
            ).start()

    def await_share(level, piece):
        rows = pl.ds(0, 80 if piece % 2 == 0 else 64)
        three = states.at[level, piece, pl.ds(0, 3), rows]
        pltpu.make_async_copy(three, three, s_recv.at[level, piece]).wait()
        pltpu.make_async_copy(three, three, s_send.at[level, piece]).wait()

    def line_decays(level, p):
        here = place[level]
        total = jnp.zeros((1, 128), F32)
        before = total
        steps = []
        for j in range(4):
            before = jnp.where(here == j, total, before)
            step = jnp.sum(states[level, 2 * p, j, 64:80, :].astype(F32), axis=0, keepdims=True)
            steps.append(jnp.exp(step))
            total = total + step
        return jnp.exp(before), total, steps

    def run_line(level, piece, steps):
        here = place[level]
        state = jnp.zeros((64, 128), F32)
        enter = state
        for j in range(4):
            enter = jnp.where(here == j, state, enter)
            state = state * steps[j] + states[level, piece, j, 0:64, :].astype(F32)
        return enter, state

    get_k.wait()
    get_v.wait()
    for p in range(PAIRS):
        local_end = state_after(SEG // BLOCK, p).astype(BF16)
        states[2, 2 * p, place[2], 0:64, :] = local_end[0:64]
        put_decays(2, p, end_row(SEG // BLOCK)[:, p * 128 : (p + 1) * 128])
        states[2, 2 * p + 1, place[2], 0:64, :] = local_end[64:128]
        if p == 0:
            pl.semaphore_wait(barrier, len(friends))
        share(2, 2 * p)
        share(2, 2 * p + 1)
    get_q.wait()
    scale = 64.0 ** (-0.5)
    block_row = iota((SEG, 1), 0) // BLOCK
    f = f_v[...]
    start = jnp.zeros((SEG, 256), F32)
    for n in range(1, SEG // BLOCK):
        start = jnp.where(block_row == n, end_row(n), start)
    running = f - start
    q = q_v[...].astype(F32) * scale
    qd_v[...] = (q * jnp.exp(f)).astype(BF16)
    q_scaled = (q * jnp.exp(running)).astype(BF16)
    k_inverse = (k_v[...].astype(F32) * jnp.exp(-running)).astype(BF16)
    row, col = iota((SEG, SEG), 0), iota((SEG, SEG), 1)
    causal = (row >= col) & (row // BLOCK == col // BLOCK)
    none = jnp.zeros((), BF16)
    local_states = [None] + [
        [state_after(n, p).astype(BF16) for p in range(PAIRS)] for n in range(1, SEG // BLOCK)
    ]
    for h in range(HEADS):
        p = h // 2
        mine = lane_low if h % 2 == 0 else jnp.logical_not(lane_low)
        lanes = slice(p * 128, (p + 1) * 128)
        q_h = jnp.where(mine, q_scaled[:, lanes], none)
        k_h = jnp.where(mine, k_inverse[:, lanes], none)
        scores = jnp.where(causal, dot(q_h, k_h, ((1,), (1,))), 0.0).astype(BF16)
        here = slice(h * 128, (h + 1) * 128)
        att_v[:, here] = dot(scores, v_v[:, here])
        for n in range(1, SEG // BLOCK):
            rows = slice(n * BLOCK, (n + 1) * BLOCK)
            att_v[rows, here] += dot(q_h[rows], local_states[n][p], ((1,), (1,)))
    get_og.wait()
    for copy in get_small:
        copy.wait()
    for h in range(HEADS):
        here = slice(h * 128, (h + 1) * 128)
        gain_v[:, here] = silu(og_v[:, here].astype(F32)) * head_gain[...]

    diagonal = iota((128, 128), 0) == iota((128, 128), 1)

    def as_column(line):
        return jnp.sum(jnp.where(diagonal, line, 0.0), axis=1, keepdims=True)

    expert_id = iota((128, 128), 0)
    earlier = jnp.where(iota((128, 128), 0) < iota((128, 128), 1), 1.0, 0.0).astype(BF16)
    taken = jnp.zeros((128, 1), F32)
    slot_rows = []
    for c in range(2):
        line = routes[c : c + 1, :]
        hit = jnp.where(expert_id == line, 1.0, 0.0)
        count = dot(hit.astype(BF16), earlier) + taken
        rank = jnp.sum(hit * count, axis=0, keepdims=True)
        offset = jnp.zeros_like(line)
        for a, unit in enumerate((32, 8, 2, 1)):
            size = 2 if a == 3 else 4
            offset = offset + unit * ((line // unit % size - place[a] + size) % size)
        step = offset * UNSTRIDE % DEVICES
        slot_rows.append((step * CAP).astype(F32) + rank)
        taken = taken + jnp.sum(hit, axis=1, keepdims=True)
    slot_id = iota((SLOTS, 128), 0).astype(F32)
    pick_v[...] = (
        jnp.where(slot_id == slot_rows[0], 1.0, 0.0) + jnp.where(slot_id == slot_rows[1], 1.0, 0.0)
    ).astype(BF16)
    score = [as_column(expert_score[c : c + 1, :]) for c in range(2)]
    group = as_column(group_score[...])
    slot_columns = [as_column(line) for line in slot_rows]
    for part in range(PARTS):
        slot_lane = (iota((ROWS, PART), 1) + part * PART).astype(F32)
        comb = jnp.zeros((ROWS, PART), F32)
        for c in range(2):
            weight = group * score[c] / (score[0] + score[1])
            comb = comb + jnp.where(slot_lane == slot_columns[c], weight, 0.0)
        high, mid, _ = split3(comb)
        comb_v[part, 0:ROWS] = mid
        comb_v[part, ROWS : 2 * ROWS] = high

    other_rows = pl.ds(pl.multiple_of((1 - core) * ROWS, ROWS), ROWS)
    own_rows = pl.ds(pl.multiple_of(core * ROWS, ROWS), ROWS)
    swaps = [
        pltpu.make_async_remote_copy(
            src_ref=mix_v.at[p, other_rows],
            dst_ref=pair_v.at[p],
            send_sem=p_send.at[p],
            recv_sem=p_recv.at[p],
            device_id=shifted(3, 1),
            device_id_type=MESH,
        )
        for p in range(PAIRS)
    ]

    def project(mixed, whose, p):
        first = pl.multiple_of(whose * (HEADS * 128) + p * 256, 256)
        return dot(mixed, ow_v[pl.ds(first, 256), :])

    entered = [[] for _ in range(2 * PAIRS)]
    for level in (2, 1, 0):
        for piece in range(2 * PAIRS):
            p = piece // 2
            await_share(level, piece)
            if piece % 2 == 0:
                scale, total, steps = line_decays(level, p)
            enter, state = run_line(level, piece, steps)
            entered[piece].append((scale, enter))
            if level:
                upper = level - 1
                states[upper, piece, place[upper], 0:64, :] = state.astype(BF16)
                if piece % 2 == 0:
                    put_decays(upper, p, total)
                share(upper, piece)
            elif piece % 2 == 1:
                halves = []
                for past in entered[piece - 1 : piece + 1]:
                    (scale_x, enter_x), (scale_y, enter_y), (_, enter_z) = past
                    halves.append(enter_x + scale_x * (enter_y + scale_y * enter_z))
                entering = jnp.concatenate(halves, axis=0).astype(BF16)
                for h in (2 * p, 2 * p + 1):
                    mine = lane_low if h % 2 == 0 else jnp.logical_not(lane_low)
                    here = slice(h * 128, (h + 1) * 128)
                    q_h = jnp.where(mine, qd_v[:, p * 128 : (p + 1) * 128], none)
                    attended = att_v[:, here] + dot(q_h, entering, ((1,), (1,)))
                    mean = jnp.mean(attended * attended, axis=-1, keepdims=True)
                    mixed = attended * lax.rsqrt(mean + 1e-06) * gain_v[:, here]
                    mix_v[p, :, (h % 2) * 128 : (h % 2 + 1) * 128] = mixed.astype(BF16)
                swaps[p].start()
                if p == 0:
                    get_res.wait()
                    get_ow.wait()
                    acc_v[...] = res_v[...].astype(F32) + project(mix_v[p, own_rows, :], core, p)
                else:
                    acc_v[...] += project(mix_v[p, own_rows, :], core, p)
    swaps[0].wait()
    acc_v[...] += project(pair_v[0], 1 - core, 0)
    swaps[1].wait()
    summed = acc_v[...] + project(pair_v[1], 1 - core, 1)
    wide = summed.astype(BF16).astype(F32)
    acc_v[...] = wide
    mean = jnp.mean(wide * wide, axis=-1, keepdims=True)
    norm_v[...] = (wide * lax.rsqrt(mean + 1e-06) * norm_gain[...]).astype(BF16)

    def put_columns(j, block):
        for i in range(2):
            tile_v[pl.ds(2 * j + i, PART, stride=PITCH), :] = block[:, i * 128 : (i + 1) * 128]

    def gather_tiles(dst, part):
        @pl.loop(0, PART // 16)
        def _(g):
            for i in range(16):
                slot = g * 16 + i
                dst[part * PART + slot] = tile_v[pl.ds(slot * PITCH, CHUNKS), :].astype(BF16)

    def to_rows(src, part):
        @pl.loop(0, PART // 32)
        def _(g):
            for i in range(2):
                rows = pl.ds(pl.multiple_of(g * 32 + i * 16, 16), 16)
                nat_v[rows, :] = src[pl.ds(part * PART + g * 32 + i * 16, 16)].reshape(16, WIDTH)

    def send_part(part, src, dst, ss, rs, sign):
        @pl.loop(max(1, part * STEPS), (part + 1) * STEPS)
        def _(i):
            offset = lax.rem(i * STRIDE, DEVICES)
            steps = (
                lax.div(offset, 32), lax.rem(lax.div(offset, 8), 4), lax.rem(lax.div(offset, 2), 4),
                lax.rem(offset, 2),
            )
            there = tuple(
                lax.rem(place[a] + sign * steps[a] + 4, 2 if a == 3 else 4) for a in range(4)
            )
            rows = pl.ds(i * CAP, CAP)
            pltpu.make_async_remote_copy(
                src_ref=src.at[rows],
                dst_ref=dst.at[rows],
                send_sem=ss,
                recv_sem=rs.at[part],
                device_id=there,
                device_id_type=MESH,
            ).start()

        if part == 0:
            dst[0:CAP] = src[0:CAP]

    def await_part(part, dst, rs):
        count = PART - (CAP if part == 0 else 0)
        rows = dst.at[pl.ds(part * PART, count)]
        pltpu.make_async_copy(rows, rows, rs.at[part]).wait()

    for part in range(PARTS):
        chosen = pick_v[part * PART : (part + 1) * PART, :]
        for j in range(WIDTH // 256):
            put_columns(j, dot(chosen, norm_v[:, j * 256 : (j + 1) * 256]))
        gather_tiles(send_v, part)
        send_part(part, send_v, recv_v, x_send, x_recv, 1)
    get_gw.wait()
    get_uw.wait()
    get_dw.wait()
    for part in range(PARTS):
        await_part(part, recv_v, x_recv)
        to_rows(recv_v, part)
        for n in range(HIDDEN // 256):
            cols = slice(n * 256, (n + 1) * 256)
            gated = dot(nat_v[...], gw_v[:, cols])
            lifted = dot(nat_v[...], uw_v[:, cols])
            inner_v[:, cols] = (silu(gated) * lifted).astype(BF16)
        for j in range(WIDTH // 256):
            put_columns(j, dot(inner_v[...], dw_v[:, j * 256 : (j + 1) * 256]))
        gather_tiles(back_v, part)
        send_part(part, back_v, ret_v, y_send, y_recv, -1)
    for part in range(PARTS):
        await_part(part, ret_v, y_recv)
        to_rows(ret_v, part)
        for j in range(WIDTH // 256):
            cols = slice(j * 256, (j + 1) * 256)
            both = dot(comb_v[part], nat_v[:, cols])
            total = acc_v[:, cols] + (both[0:ROWS] + both[ROWS : 2 * ROWS])
            if part < PARTS - 1:
                acc_v[:, cols] = total
            else:
                out[:, cols] = total.astype(BF16)
    for src, ss in ((send_v, x_send), (back_v, y_send)):
        rows = src.at[pl.ds(0, SLOTS - CAP)]
        pltpu.make_async_copy(rows, rows, ss).wait()


def local(
    residual, queries, key_rows, value_rows, out_gate, gate_logits, head_gain, out_weight,
    norm_gain, routes, group_score, expert_score, gate_weight, up_weight, down_weight,
):
    anywhere = pl.BlockSpec(memory_space=pl.ANY)
    vmem = pl.BlockSpec(memory_space=pltpu.VMEM)
    half = HEADS * 128
    tiles = pltpu.VMEM((SLOTS, CHUNKS, 128), BF16)
    dma = pltpu.SemaphoreType.DMA
    return pl.pallas_call(
        kernel,
        out_shape=pltpu.VMEM((ROWS, WIDTH), BF16),
        in_specs=[anywhere] * 15,
        out_specs=vmem,
        scratch_shapes=[
            pltpu.VMEM((1, 128), F32),
            pltpu.VMEM((1, WIDTH), F32),
            pltpu.VMEM((2, ROWS), I32),
            pltpu.VMEM((1, ROWS), F32),
            pltpu.VMEM((2, ROWS), F32),
            pltpu.VMEM((SEG, 256), BF16),
            pltpu.VMEM((SEG, 256), BF16),
            pltpu.VMEM((SEG, half), BF16),
            pltpu.VMEM((SEG, half), BF16),
            pltpu.VMEM((SEG, 256), BF16),
            pltpu.VMEM((ROWS, WIDTH), BF16),
            pltpu.VMEM((2 * half, WIDTH), BF16),
            pltpu.VMEM((WIDTH, HIDDEN), BF16),
            pltpu.VMEM((WIDTH, HIDDEN), BF16),
            pltpu.VMEM((HIDDEN, WIDTH), BF16),
            pltpu.VMEM((SEG, 256), F32),
            pltpu.VMEM((SEG, 256), BF16),
            pltpu.VMEM((SEG, half), F32),
            pltpu.VMEM((SEG, half), F32),
            pltpu.VMEM((PAIRS, SEG, 256), BF16),
            pltpu.VMEM((PAIRS, ROWS, 256), BF16),
            pltpu.VMEM((3, 2 * PAIRS, 4, 80, 128), BF16),
            pltpu.VMEM((SLOTS, ROWS), BF16),
            pltpu.VMEM((PARTS, 2 * ROWS, PART), BF16),
            pltpu.VMEM((ROWS, WIDTH), BF16),
            pltpu.VMEM((ROWS, WIDTH), F32),
            pltpu.VMEM((PART, WIDTH), BF16),
            pltpu.VMEM((PART * PITCH, 128), F32),
            tiles,
            tiles,
            pltpu.VMEM((PART, HIDDEN), BF16),
            tiles,
            tiles,
            dma((11,)), dma((4,)),
            dma((3, 2 * PAIRS)), dma((3, 2 * PAIRS)),
            dma((PAIRS,)), dma((PAIRS,)), dma, dma((PARTS,)), dma, dma((PARTS,)),
        ],
        compiler_params=pltpu.CompilerParams(
            collective_id=0, has_side_effects=True, vmem_limit_bytes=56 * 2**20
        ),
    )(
        residual, queries, key_rows, value_rows, out_gate, gate_logits,
        head_gain.reshape(1, 128), out_weight, norm_gain.reshape(1, WIDTH),
        routes.T, group_score.reshape(1, ROWS), expert_score.T, gate_weight, up_weight, down_weight,
    )


def solution(mesh):
    torus = Mesh(mesh.devices.reshape(4, 4, 4, mesh.shape["tp"]), AXES)
    both = P(AXES)
    in_specs = (
        P(AXES, None),
        P(SP, "tp"), P(SP, "tp"), P(SP, "tp"), P(SP, "tp"), P(SP, "tp"),
        P(), P(), P(),
        P(AXES, None), both, P(AXES, None),
        P(AXES, None, None), P(AXES, None, None), P(AXES, None, None),
    )
    return jax.shard_map(
        local, mesh=torus, in_specs=in_specs, out_specs=P(AXES, None), check_vma=False
    )
```

```python
import jax
import jax.numpy as jnp
from jax import lax
from jax.experimental import pallas as pl
from jax.experimental.pallas import tpu as pltpu
from jax.sharding import Mesh
from jax.sharding import PartitionSpec as P

AXES = ("sp_0", "sp_1", "sp_2", "tp")
SP = AXES[:3]
MESH = pl.DeviceIdType.MESH
F32, BF16, I32 = jnp.float32, jnp.bfloat16, jnp.int32

BLOCK = 64
SEG = 256
ROWS = 128
HEADS = 4
PAIRS = HEADS // 2
SPLIT = 4
PIECES = PAIRS * SPLIT
PIECE = 128 // SPLIT
WIDTH = 2048
CHUNKS = WIDTH // 128
HIDDEN = 512
DEVICES = 128
CAP = 3
SLOTS = DEVICES * CAP
BOUNDS = (0, 32, 64, 96, 128)
PARTS = len(BOUNDS) - 1
SIZES = [(BOUNDS[i + 1] - BOUNDS[i]) * CAP for i in range(PARTS)]
PART = max(SIZES)
STRIDE, UNSTRIDE = 53, 29
PITCH = CHUNKS + 1


def dot(a, b, dims=((1,), (0,))):
    return lax.dot_general(a, b, (dims, ((), ())), preferred_element_type=F32)


def split3(x):
    high = x.astype(BF16)
    rest = x - high.astype(F32)
    mid = rest.astype(BF16)
    return high, mid, (rest - mid.astype(F32)).astype(BF16)


def split2(x):
    high = x.astype(BF16)
    return high, (x - high.astype(F32)).astype(BF16)


def dot_split(a, b, dims=((1,), (0,))):
    return dot(a[0], b[0], dims) + (dot(a[0], b[1], dims) + dot(a[1], b[0], dims))


def iota(shape, dim):
    return lax.broadcasted_iota(I32, shape, dim)


def silu(x):
    return x / (1.0 + jnp.exp(-x))


def kernel(
    residual, queries, keys, values, out_gate, gate_logits, head_gain_h, out_weight, norm_gain_h,
    routes_h, group_score_h, expert_score_h, gate_weight, up_weight, down_weight,
    out,
    head_gain, norm_gain, routes, group_score, expert_score,
    q_v, k_v, v_v, og_v, gl_v, res_v, ow_v, gw_v, uw_v, dw_v,
    f_v, qd_v, att_v, gain_v, mix_v, pair_v, states, pick_v, comb_v,
    norm_v, acc_v, nat_v, tile_v, send_v, recv_v, inner_v, back_v, ret_v,
    in_sem, w_sem, s_send, s_recv, p_send, p_recv, x_send, x_recv, y_send, y_recv,
):
    place = [lax.axis_index(axis) for axis in AXES]
    core = place[3]
    me = ((place[0] * 4 + place[1]) * 4 + place[2]) * 2 + core

    def shifted(axis, step):
        there = list(place)
        size = 2 if axis == 3 else 4
        there[axis] = (place[axis] + step) % size
        return tuple(there)

    def fetch(pairs, sems, first):
        copies = [
            pltpu.make_async_copy(src, dst, sems.at[first + i]) for i, (src, dst) in enumerate(pairs)
        ]
        for copy in copies:
            copy.start()
        return copies

    get_gl, get_k, get_v, get_q, get_og, get_res = fetch(
        (
            (gate_logits, gl_v), (keys, k_v), (values, v_v), (queries, q_v), (out_gate, og_v),
            (residual, res_v),
        ),
        in_sem,
        0,
    )
    get_small = fetch(
        (
            (head_gain_h, head_gain), (norm_gain_h, norm_gain), (routes_h, routes),
            (group_score_h, group_score), (expert_score_h, expert_score),
        ),
        in_sem,
        6,
    )
    get_ow, get_gw, get_uw, get_dw = fetch(
        (
            (out_weight, ow_v), (gate_weight.at[0], gw_v), (up_weight.at[0], uw_v),
            (down_weight.at[0], dw_v),
        ),
        w_sem,
        0,
    )

    barrier = pltpu.get_barrier_semaphore()
    friends = [(axis, step) for axis in range(3) for step in (1, 2, 3)] + [(3, 1)]
    for axis, step in friends:
        pl.semaphore_signal(
            barrier, inc=1, device_id=shifted(axis, step), device_id_type=MESH
        )

    get_gl.wait()
    x = -gl_v[...].astype(F32)
    decay = -(jnp.maximum(x, 0.0) + jnp.log1p(jnp.exp(-jnp.abs(x)))) * (1.0 / 16.0)
    lower = jnp.where(iota((SEG, SEG), 0) >= iota((SEG, SEG), 1), 1.0, 0.0).astype(BF16)
    high, mid, low = split3(decay)
    f_v[...] = (dot(lower, low) + dot(lower, mid)) + dot(lower, high)

    def end_row(n):
        return f_v[pl.ds(n * BLOCK - 1, 1), :]

    lane_low = iota((1, 128), 1) < 64

    def state_after(n, p):
        rows, lanes = n * BLOCK, slice(p * 128, (p + 1) * 128)
        aged = k_v[0:rows, lanes].astype(F32) * jnp.exp(end_row(n)[:, lanes] - f_v[0:rows, lanes])
        side = []
        for i in range(2):
            v_h = v_v[0:rows, (2 * p + i) * 128 : (2 * p + i + 1) * 128]
            side.append(sum(dot(v_h, part, ((0,), (0,))) for part in split2(aged)))
        return jnp.where(lane_low, side[0], side[1])

    def put_decays(level, lines):
        part_row = iota((16, 128), 0)
        rows = jnp.zeros((16, 128), F32)
        for p in range(PAIRS):
            for i, part in enumerate(split3(lines[p])):
                rows = jnp.where(part_row == 3 * p + i, part.astype(F32), rows)
        states[level, 0, place[level], PIECE : PIECE + 16, :] = rows.astype(BF16)

    def piece_rows(piece):
        return pl.ds(0, PIECE + 16 if piece == 0 else PIECE)

    def share(level, piece):
        here = place[level]
        for step in (2, 1, 3):
            pltpu.make_async_remote_copy(
                src_ref=states.at[level, piece, here, piece_rows(piece)],
                dst_ref=states.at[level, piece, here, piece_rows(piece)],
                send_sem=s_send.at[level, piece],
                recv_sem=s_recv.at[level, piece],
                device_id=shifted(level, step),
                device_id_type=MESH,
            ).start()

    def await_share(level, piece):
        three = states.at[level, piece, pl.ds(0, 3), piece_rows(piece)]
        pltpu.make_async_copy(three, three, s_recv.at[level, piece]).wait()
        pltpu.make_async_copy(three, three, s_send.at[level, piece]).wait()

    def line_decays(level, p):
        here = place[level]
        total = jnp.zeros((1, 128), F32)
        before = total
        steps = []
        for j in range(4):
            before = jnp.where(here == j, total, before)
            parts = states[level, 0, j, PIECE : PIECE + 16, :].astype(F32)
            step = (parts[3 * p + 2 : 3 * p + 3] + parts[3 * p + 1 : 3 * p + 2]) + parts[3 * p : 3 * p + 1]
            steps.append(jnp.exp(step))
            total = total + step
        return jnp.exp(before), total, steps

    def run_line(level, piece, steps):
        here = place[level]
        state = jnp.zeros((PIECE, 128), F32)
        enter = state
        for j in range(4):
            enter = jnp.where(here == j, state, enter)
            state = state * steps[j] + states[level, piece, j, 0:PIECE, :].astype(F32)
        return enter, state

    get_k.wait()
    get_v.wait()
    whole = end_row(SEG // BLOCK)
    put_decays(2, [whole[:, p * 128 : (p + 1) * 128] for p in range(PAIRS)])
    for p in range(PAIRS):
        local_end = state_after(SEG // BLOCK, p).astype(BF16)
        for i in range(SPLIT):
            states[2, p * SPLIT + i, place[2], 0:PIECE, :] = local_end[i * PIECE : (i + 1) * PIECE]
        if p == 0:
            pl.semaphore_wait(barrier, len(friends))
        for i in range(SPLIT):
            share(2, p * SPLIT + i)
    get_q.wait()
    scale = 64.0 ** (-0.5)
    block_row = iota((SEG, 1), 0) // BLOCK
    f = f_v[...]
    start = jnp.zeros((SEG, 256), F32)
    for n in range(1, SEG // BLOCK):
        start = jnp.where(block_row == n, end_row(n), start)
    running = f - start
    q = q_v[...].astype(F32) * scale
    for i, part in enumerate(split2(q * jnp.exp(f))):
        qd_v[i] = part
    q_scaled = split2(q * jnp.exp(running))
    k_inverse = split2(k_v[...].astype(F32) * jnp.exp(-running))
    row, col = iota((SEG, SEG), 0), iota((SEG, SEG), 1)
    causal = (row >= col) & (row // BLOCK == col // BLOCK)
    none = jnp.zeros((), BF16)
    local_states = [None] + [
        [split2(state_after(n, p)) for p in range(PAIRS)] for n in range(1, SEG // BLOCK)
    ]
    for h in range(HEADS):
        p = h // 2
        mine = lane_low if h % 2 == 0 else jnp.logical_not(lane_low)
        lanes = slice(p * 128, (p + 1) * 128)
        q_h = [jnp.where(mine, part[:, lanes], none) for part in q_scaled]
        k_h = [jnp.where(mine, part[:, lanes], none) for part in k_inverse]
        scores = jnp.where(causal, dot_split(q_h, k_h, ((1,), (1,))), 0.0)
        here = slice(h * 128, (h + 1) * 128)
        att_v[:, here] = sum(dot(part, v_v[:, here]) for part in split2(scores))
        for n in range(1, SEG // BLOCK):
            rows = slice(n * BLOCK, (n + 1) * BLOCK)
            q_n = [part[rows] for part in q_h]
            att_v[rows, here] += dot_split(q_n, local_states[n][p], ((1,), (1,)))
    get_og.wait()
    for copy in get_small:
        copy.wait()
    for h in range(HEADS):
        here = slice(h * 128, (h + 1) * 128)
        gain_v[:, here] = silu(og_v[:, here].astype(F32)) * head_gain[...]

    diagonal = iota((128, 128), 0) == iota((128, 128), 1)

    def as_column(line):
        return jnp.sum(jnp.where(diagonal, line, 0.0), axis=1, keepdims=True)

    expert_id = iota((128, 128), 0)
    earlier = jnp.where(iota((128, 128), 0) < iota((128, 128), 1), 1.0, 0.0).astype(BF16)
    taken = jnp.zeros((128, 1), F32)
    slot_rows = []
    for c in range(2):
        line = routes[c : c + 1, :]
        hit = jnp.where(expert_id == line, 1.0, 0.0)
        count = dot(hit.astype(BF16), earlier) + taken
        rank = jnp.sum(hit * count, axis=0, keepdims=True)
        offset = jnp.zeros_like(line)
        for a, unit in enumerate((32, 8, 2, 1)):
            size = 2 if a == 3 else 4
            offset = offset + unit * ((line // unit % size - place[a] + size) % size)
        step = offset * UNSTRIDE % DEVICES
        slot_rows.append((step * CAP).astype(F32) + rank)
        taken = taken + jnp.sum(hit, axis=1, keepdims=True)
    slot_id = iota((SLOTS, 128), 0).astype(F32)
    pick_v[...] = (
        jnp.where(slot_id == slot_rows[0], 1.0, 0.0) + jnp.where(slot_id == slot_rows[1], 1.0, 0.0)
    ).astype(BF16)
    score = [as_column(expert_score[c : c + 1, :]) for c in range(2)]
    group = as_column(group_score[...])
    slot_columns = [as_column(line) for line in slot_rows]
    for part, size in enumerate(SIZES):
        slot_lane = (iota((ROWS, size), 1) + BOUNDS[part] * CAP).astype(F32)
        comb = jnp.zeros((ROWS, size), F32)
        for c in range(2):
            weight = group * score[c] / (score[0] + score[1])
            comb = comb + jnp.where(slot_lane == slot_columns[c], weight, 0.0)
        high, mid, _ = split3(comb)
        comb_v[part, 0:ROWS, 0:size] = mid
        comb_v[part, ROWS : 2 * ROWS, 0:size] = high

    other_rows = pl.ds(pl.multiple_of((1 - core) * ROWS, ROWS), ROWS)
    own_rows = pl.ds(pl.multiple_of(core * ROWS, ROWS), ROWS)
    swaps = [
        pltpu.make_async_remote_copy(
            src_ref=mix_v.at[p, other_rows],
            dst_ref=pair_v.at[p],
            send_sem=p_send.at[p],
            recv_sem=p_recv.at[p],
            device_id=shifted(3, 1),
            device_id_type=MESH,
        )
        for p in range(PAIRS)
    ]

    def project(mixed, whose, p):
        first = pl.multiple_of(whose * (HEADS * 128) + p * 256, 256)
        return dot(mixed, ow_v[pl.ds(first, 256), :])

    entered = [[] for _ in range(PIECES)]
    for level in (2, 1, 0):
        for piece in range(PIECES):
            p = piece // SPLIT
            await_share(level, piece)
            if piece == 0:
                lines = [line_decays(level, pair) for pair in range(PAIRS)]
            scale, total, steps = lines[p]
            enter, state = run_line(level, piece, steps)
            entered[piece].append((scale, enter))
            if level:
                upper = level - 1
                states[upper, piece, place[upper], 0:PIECE, :] = state.astype(BF16)
                if piece == 0:
                    put_decays(upper, [line[1] for line in lines])
                share(upper, piece)
            elif piece % SPLIT == SPLIT - 1:
                parts = []
                for past in entered[piece + 1 - SPLIT : piece + 1]:
                    (scale_x, enter_x), (scale_y, enter_y), (_, enter_z) = past
                    parts.append(enter_x + scale_x * (enter_y + scale_y * enter_z))
                entering = split2(jnp.concatenate(parts, axis=0))
                for h in (2 * p, 2 * p + 1):
                    mine = lane_low if h % 2 == 0 else jnp.logical_not(lane_low)
                    here = slice(h * 128, (h + 1) * 128)
                    q_h = [
                        jnp.where(mine, qd_v[i, :, p * 128 : (p + 1) * 128], none) for i in range(2)
                    ]
                    attended = att_v[:, here] + dot_split(q_h, entering, ((1,), (1,)))
                    mean = jnp.mean(attended * attended, axis=-1, keepdims=True)
                    mixed = attended * lax.rsqrt(mean + 1e-06) * gain_v[:, here]
                    mix_v[p, :, (h % 2) * 128 : (h % 2 + 1) * 128] = mixed.astype(BF16)
                swaps[p].start()
                if p == 0:
                    get_res.wait()
                    get_ow.wait()
                    acc_v[...] = res_v[...].astype(F32) + project(mix_v[p, own_rows, :], core, p)
                else:
                    acc_v[...] += project(mix_v[p, own_rows, :], core, p)
    swaps[0].wait()
    acc_v[...] += project(pair_v[0], 1 - core, 0)
    swaps[1].wait()
    summed = acc_v[...] + project(pair_v[1], 1 - core, 1)
    wide = summed.astype(BF16).astype(F32)
    acc_v[...] = wide
    mean = jnp.mean(wide * wide, axis=-1, keepdims=True)
    norm_v[...] = (wide * lax.rsqrt(mean + 1e-06) * norm_gain[...]).astype(BF16)

    def put_columns(j, block):
        for i in range(2):
            tile_v[pl.ds(2 * j + i, block.shape[0], stride=PITCH), :] = block[
                :, i * 128 : (i + 1) * 128
            ]

    def gather_tiles(dst, part):
        @pl.loop(0, SIZES[part] // 16)
        def _(g):
            for i in range(16):
                slot = g * 16 + i
                dst[BOUNDS[part] * CAP + slot] = tile_v[pl.ds(slot * PITCH, CHUNKS), :].astype(BF16)

    def to_rows(src, part):
        for g in range(SIZES[part] // 16):
            rows = src[BOUNDS[part] * CAP + g * 16 : BOUNDS[part] * CAP + (g + 1) * 16]
            nat_v[g * 16 : (g + 1) * 16, :] = rows.reshape(16, WIDTH)

    def send_part(part, src, dst, ss, rs, sign):
        @pl.loop(max(1, BOUNDS[part]), BOUNDS[part + 1])
        def _(i):
            offset = lax.rem(i * STRIDE, DEVICES)
            steps = (
                lax.div(offset, 32), lax.rem(lax.div(offset, 8), 4), lax.rem(lax.div(offset, 2), 4),
                lax.rem(offset, 2),
            )
            there = tuple(
                lax.rem(place[a] + sign * steps[a] + 4, 2 if a == 3 else 4) for a in range(4)
            )
            rows = pl.ds(i * CAP, CAP)
            pltpu.make_async_remote_copy(
                src_ref=src.at[rows],
                dst_ref=dst.at[rows],
                send_sem=ss,
                recv_sem=rs.at[part],
                device_id=there,
                device_id_type=MESH,
            ).start()

        if part == 0:
            dst[0:CAP] = src[0:CAP]

    def await_part(part, dst, rs):
        count = SIZES[part] - (CAP if part == 0 else 0)
        rows = dst.at[pl.ds(BOUNDS[part] * CAP, count)]
        pltpu.make_async_copy(rows, rows, rs.at[part]).wait()

    for part in range(PARTS):
        chosen = pick_v[BOUNDS[part] * CAP : BOUNDS[part + 1] * CAP, :]
        for j in range(WIDTH // 256):
            put_columns(j, dot(chosen, norm_v[:, j * 256 : (j + 1) * 256]))
        gather_tiles(send_v, part)
        send_part(part, send_v, recv_v, x_send, x_recv, 1)
    get_gw.wait()
    get_uw.wait()
    get_dw.wait()
    for part in range(PARTS):
        await_part(part, recv_v, x_recv)
        size = SIZES[part]
        to_rows(recv_v, part)
        for n in range(HIDDEN // 256):
            cols = slice(n * 256, (n + 1) * 256)
            gated = dot(nat_v[0:size, :], gw_v[:, cols])
            lifted = dot(nat_v[0:size, :], uw_v[:, cols])
            inner_v[0:size, cols] = (silu(gated) * lifted).astype(BF16)
        for j in range(WIDTH // 256):
            put_columns(j, dot(inner_v[0:size, :], dw_v[:, j * 256 : (j + 1) * 256]))
        gather_tiles(back_v, part)
        send_part(part, back_v, ret_v, y_send, y_recv, -1)
    for part in range(PARTS):
        await_part(part, ret_v, y_recv)
        size = SIZES[part]
        to_rows(ret_v, part)
        for j in range(WIDTH // 256):
            cols = slice(j * 256, (j + 1) * 256)
            both = dot(comb_v[part, :, 0:size], nat_v[0:size, cols])
            total = acc_v[:, cols] + (both[0:ROWS] + both[ROWS : 2 * ROWS])
            if part < PARTS - 1:
                acc_v[:, cols] = total
            else:
                out[:, cols] = total.astype(BF16)
    for src, ss in ((send_v, x_send), (back_v, y_send)):
        rows = src.at[pl.ds(0, SLOTS - CAP)]
        pltpu.make_async_copy(rows, rows, ss).wait()


def local(
    residual, queries, key_rows, value_rows, out_gate, gate_logits, head_gain, out_weight,
    norm_gain, routes, group_score, expert_score, gate_weight, up_weight, down_weight,
):
    anywhere = pl.BlockSpec(memory_space=pl.ANY)
    vmem = pl.BlockSpec(memory_space=pltpu.VMEM)
    half = HEADS * 128
    tiles = pltpu.VMEM((SLOTS, CHUNKS, 128), BF16)
    dma = pltpu.SemaphoreType.DMA
    return pl.pallas_call(
        kernel,
        out_shape=pltpu.VMEM((ROWS, WIDTH), BF16),
        in_specs=[anywhere] * 15,
        out_specs=vmem,
        scratch_shapes=[
            pltpu.VMEM((1, 128), F32),
            pltpu.VMEM((1, WIDTH), F32),
            pltpu.VMEM((2, ROWS), I32),
            pltpu.VMEM((1, ROWS), F32),
            pltpu.VMEM((2, ROWS), F32),
            pltpu.VMEM((SEG, 256), BF16),
            pltpu.VMEM((SEG, 256), BF16),
            pltpu.VMEM((SEG, half), BF16),
            pltpu.VMEM((SEG, half), BF16),
            pltpu.VMEM((SEG, 256), BF16),
            pltpu.VMEM((ROWS, WIDTH), BF16),
            pltpu.VMEM((2 * half, WIDTH), BF16),
            pltpu.VMEM((WIDTH, HIDDEN), BF16),
            pltpu.VMEM((WIDTH, HIDDEN), BF16),
            pltpu.VMEM((HIDDEN, WIDTH), BF16),
            pltpu.VMEM((SEG, 256), F32),
            pltpu.VMEM((2, SEG, 256), BF16),
            pltpu.VMEM((SEG, half), F32),
            pltpu.VMEM((SEG, half), F32),
            pltpu.VMEM((PAIRS, SEG, 256), BF16),
            pltpu.VMEM((PAIRS, ROWS, 256), BF16),
            pltpu.VMEM((3, PIECES, 4, PIECE + 16, 128), BF16),
            pltpu.VMEM((SLOTS, ROWS), BF16),
            pltpu.VMEM((PARTS, 2 * ROWS, PART), BF16),
            pltpu.VMEM((ROWS, WIDTH), BF16),
            pltpu.VMEM((ROWS, WIDTH), F32),
            pltpu.VMEM((PART, WIDTH), BF16),
            pltpu.VMEM((PART * PITCH, 128), F32),
            tiles,
            tiles,
            pltpu.VMEM((PART, HIDDEN), BF16),
            tiles,
            tiles,
            dma((11,)), dma((4,)),
            dma((3, PIECES)), dma((3, PIECES)),
            dma((PAIRS,)), dma((PAIRS,)), dma, dma((PARTS,)), dma, dma((PARTS,)),
        ],
        compiler_params=pltpu.CompilerParams(
            collective_id=0, has_side_effects=True, vmem_limit_bytes=56 * 2**20
        ),
    )(
        residual, queries, key_rows, value_rows, out_gate, gate_logits,
        head_gain.reshape(1, 128), out_weight, norm_gain.reshape(1, WIDTH),
        routes.T, group_score.reshape(1, ROWS), expert_score.T, gate_weight, up_weight, down_weight,
    )


def solution(mesh):
    torus = Mesh(mesh.devices.reshape(4, 4, 4, mesh.shape["tp"]), AXES)
    both = P(AXES)
    in_specs = (
        P(AXES, None),
        P(SP, "tp"), P(SP, "tp"), P(SP, "tp"), P(SP, "tp"), P(SP, "tp"),
        P(), P(), P(),
        P(AXES, None), both, P(AXES, None),
        P(AXES, None, None), P(AXES, None, None), P(AXES, None, None),
    )
    return jax.shard_map(
        local, mesh=torus, in_specs=in_specs, out_specs=P(AXES, None), check_vma=False
    )
```

```python
import jax
import jax.numpy as jnp
from jax import lax
from jax.experimental import pallas as pl
from jax.experimental.pallas import tpu as pltpu
from jax.sharding import Mesh
from jax.sharding import PartitionSpec as P

AXES = ("sp_0", "sp_1", "sp_2", "tp")
SP = AXES[:3]
MESH = pl.DeviceIdType.MESH
F32, BF16, I32 = jnp.float32, jnp.bfloat16, jnp.int32

BLOCK = 64
SEG = 256
ROWS = 128
HEADS = 4
PAIRS = HEADS // 2
SPLIT = 4
PIECES = PAIRS * SPLIT
PIECE = 128 // SPLIT
WIDTH = 2048
CHUNKS = WIDTH // 128
HIDDEN = 512
DEVICES = 128
CAP = 3
SLOTS = DEVICES * CAP
BOUNDS = (0, 32, 64, 96, 128)
PARTS = len(BOUNDS) - 1
SIZES = [(BOUNDS[i + 1] - BOUNDS[i]) * CAP for i in range(PARTS)]
PART = max(SIZES)
STRIDE, UNSTRIDE = 91, 83
PITCH = CHUNKS + 1


def dot(a, b, dims=((1,), (0,))):
    return lax.dot_general(a, b, (dims, ((), ())), preferred_element_type=F32)


def split3(x):
    high = x.astype(BF16)
    rest = x - high.astype(F32)
    mid = rest.astype(BF16)
    return high, mid, (rest - mid.astype(F32)).astype(BF16)


def split2(x):
    high = x.astype(BF16)
    return high, (x - high.astype(F32)).astype(BF16)


def dot_split(a, b, dims=((1,), (0,))):
    return dot(a[0], b[0], dims) + (dot(a[0], b[1], dims) + dot(a[1], b[0], dims))


def iota(shape, dim):
    return lax.broadcasted_iota(I32, shape, dim)


def silu(x):
    return x / (1.0 + jnp.exp(-x))


def kernel(
    residual, queries, keys, values, out_gate, gate_logits, head_gain_h, out_weight, norm_gain_h,
    routes_h, group_score_h, expert_score_h, gate_weight, up_weight, down_weight,
    out,
    head_gain, norm_gain, routes, group_score, expert_score,
    q_v, k_v, v_v, og_v, gl_v, res_v, ow_v, gw_v, uw_v, dw_v,
    f_v, qd_v, att_v, gain_v, mix_v, pair_v, states, pick_v, comb_v,
    norm_v, acc_v, nat_v, tile_v, send_v, recv_v, inner_v, back_v, ret_v,
    in_sem, w_sem, s_send, s_recv, p_send, p_recv, x_send, x_recv, y_send, y_recv,
):
    place = [lax.axis_index(axis) for axis in AXES]
    core = place[3]
    me = ((place[0] * 4 + place[1]) * 4 + place[2]) * 2 + core

    def shifted(axis, step):
        there = list(place)
        size = 2 if axis == 3 else 4
        there[axis] = (place[axis] + step) % size
        return tuple(there)

    def fetch(pairs, sems, first):
        copies = [
            pltpu.make_async_copy(src, dst, sems.at[first + i]) for i, (src, dst) in enumerate(pairs)
        ]
        for copy in copies:
            copy.start()
        return copies

    get_gl, get_k, get_v, get_q, get_og, get_res = fetch(
        (
            (gate_logits, gl_v), (keys, k_v), (values, v_v), (queries, q_v), (out_gate, og_v),
            (residual, res_v),
        ),
        in_sem,
        0,
    )
    get_small = fetch(
        (
            (head_gain_h, head_gain), (norm_gain_h, norm_gain), (routes_h, routes),
            (group_score_h, group_score), (expert_score_h, expert_score),
        ),
        in_sem,
        6,
    )
    get_ow, get_gw, get_uw, get_dw = fetch(
        (
            (out_weight, ow_v), (gate_weight.at[0], gw_v), (up_weight.at[0], uw_v),
            (down_weight.at[0], dw_v),
        ),
        w_sem,
        0,
    )

    barrier = pltpu.get_barrier_semaphore()
    friends = [(axis, step) for axis in range(3) for step in (1, 2, 3)] + [(3, 1)]
    for axis, step in friends:
        pl.semaphore_signal(
            barrier, inc=1, device_id=shifted(axis, step), device_id_type=MESH
        )

    get_gl.wait()
    x = -gl_v[...].astype(F32)
    decay = -(jnp.maximum(x, 0.0) + jnp.log1p(jnp.exp(-jnp.abs(x)))) * (1.0 / 16.0)
    lower = jnp.where(iota((SEG, SEG), 0) >= iota((SEG, SEG), 1), 1.0, 0.0).astype(BF16)
    high, mid, low = split3(decay)
    f_v[...] = (dot(lower, low) + dot(lower, mid)) + dot(lower, high)

    def end_row(n):
        return f_v[pl.ds(n * BLOCK - 1, 1), :]

    lane_low = iota((1, 128), 1) < 64

    def state_after(n, p):
        rows, lanes = n * BLOCK, slice(p * 128, (p + 1) * 128)
        aged = k_v[0:rows, lanes].astype(F32) * jnp.exp(end_row(n)[:, lanes] - f_v[0:rows, lanes])
        side = []
        for i in range(2):
            v_h = v_v[0:rows, (2 * p + i) * 128 : (2 * p + i + 1) * 128]
            side.append(sum(dot(v_h, part, ((0,), (0,))) for part in split2(aged)))
        return jnp.where(lane_low, side[0], side[1])

    def put_decays(level, lines):
        part_row = iota((16, 128), 0)
        rows = jnp.zeros((16, 128), F32)
        for p in range(PAIRS):
            for i, part in enumerate(split3(lines[p])):
                rows = jnp.where(part_row == 3 * p + i, part.astype(F32), rows)
        states[level, 0, place[level], PIECE : PIECE + 16, :] = rows.astype(BF16)

    def piece_rows(piece):
        return pl.ds(0, PIECE + 16 if piece == 0 else PIECE)

    def share(level, piece):
        here = place[level]
        for step in (2, 1, 3):
            pltpu.make_async_remote_copy(
                src_ref=states.at[level, piece, here, piece_rows(piece)],
                dst_ref=states.at[level, piece, here, piece_rows(piece)],
                send_sem=s_send,
                recv_sem=s_recv.at[level, piece],
                device_id=shifted(level, step),
                device_id_type=MESH,
            ).start()

    def await_share(level, piece):
        three = states.at[level, piece, pl.ds(0, 3), piece_rows(piece)]
        pltpu.make_async_copy(three, three, s_recv.at[level, piece]).wait()

    def line_decays(level, p):
        here = place[level]
        total = jnp.zeros((1, 128), F32)
        before = total
        steps = []
        for j in range(4):
            before = jnp.where(here == j, total, before)
            parts = states[level, 0, j, PIECE : PIECE + 16, :].astype(F32)
            step = (parts[3 * p + 2 : 3 * p + 3] + parts[3 * p + 1 : 3 * p + 2]) + parts[3 * p : 3 * p + 1]
            steps.append(jnp.exp(step))
            total = total + step
        return jnp.exp(before), total, steps

    def run_line(level, piece, steps):
        here = place[level]
        state = jnp.zeros((PIECE, 128), F32)
        enter = state
        for j in range(4):
            enter = jnp.where(here == j, state, enter)
            state = state * steps[j] + states[level, piece, j, 0:PIECE, :].astype(F32)
        return enter, state

    get_k.wait()
    get_v.wait()
    whole = end_row(SEG // BLOCK)
    put_decays(2, [whole[:, p * 128 : (p + 1) * 128] for p in range(PAIRS)])
    for p in range(PAIRS):
        local_end = state_after(SEG // BLOCK, p).astype(BF16)
        for i in range(SPLIT):
            states[2, p * SPLIT + i, place[2], 0:PIECE, :] = local_end[i * PIECE : (i + 1) * PIECE]
        if p == 0:
            pl.semaphore_wait(barrier, len(friends))
        for i in range(SPLIT):
            share(2, p * SPLIT + i)
    get_q.wait()
    scale = 64.0 ** (-0.5)
    block_row = iota((SEG, 1), 0) // BLOCK
    f = f_v[...]
    start = jnp.zeros((SEG, 256), F32)
    for n in range(1, SEG // BLOCK):
        start = jnp.where(block_row == n, end_row(n), start)
    running = f - start
    q = q_v[...].astype(F32) * scale
    for i, part in enumerate(split2(q * jnp.exp(f))):
        qd_v[i] = part
    q_scaled = split2(q * jnp.exp(running))
    k_inverse = split2(k_v[...].astype(F32) * jnp.exp(-running))
    row, col = iota((SEG, SEG), 0), iota((SEG, SEG), 1)
    causal = (row >= col) & (row // BLOCK == col // BLOCK)
    none = jnp.zeros((), BF16)
    local_states = [None] + [
        [split2(state_after(n, p)) for p in range(PAIRS)] for n in range(1, SEG // BLOCK)
    ]
    for h in range(HEADS):
        p = h // 2
        mine = lane_low if h % 2 == 0 else jnp.logical_not(lane_low)
        lanes = slice(p * 128, (p + 1) * 128)
        q_h = [jnp.where(mine, part[:, lanes], none) for part in q_scaled]
        k_h = [jnp.where(mine, part[:, lanes], none) for part in k_inverse]
        scores = jnp.where(causal, dot_split(q_h, k_h, ((1,), (1,))), 0.0)
        here = slice(h * 128, (h + 1) * 128)
        att_v[:, here] = sum(dot(part, v_v[:, here]) for part in split2(scores))
        for n in range(1, SEG // BLOCK):
            rows = slice(n * BLOCK, (n + 1) * BLOCK)
            q_n = [part[rows] for part in q_h]
            att_v[rows, here] += dot_split(q_n, local_states[n][p], ((1,), (1,)))
    get_og.wait()
    for copy in get_small:
        copy.wait()
    for h in range(HEADS):
        here = slice(h * 128, (h + 1) * 128)
        gain_v[:, here] = silu(og_v[:, here].astype(F32)) * head_gain[...]

    diagonal = iota((128, 128), 0) == iota((128, 128), 1)

    def as_column(line):
        return jnp.sum(jnp.where(diagonal, line, 0.0), axis=1, keepdims=True)

    expert_id = iota((128, 128), 0)
    earlier = jnp.where(iota((128, 128), 0) < iota((128, 128), 1), 1.0, 0.0).astype(BF16)
    taken = jnp.zeros((128, 1), F32)
    slot_rows = []
    for c in range(2):
        line = routes[c : c + 1, :]
        hit = jnp.where(expert_id == line, 1.0, 0.0)
        count = dot(hit.astype(BF16), earlier) + taken
        rank = jnp.sum(hit * count, axis=0, keepdims=True)
        offset = jnp.zeros_like(line)
        for a, unit in enumerate((32, 8, 2, 1)):
            size = 2 if a == 3 else 4
            offset = offset + unit * ((line // unit % size - place[a] + size) % size)
        step = offset * UNSTRIDE % DEVICES
        slot_rows.append((step * CAP).astype(F32) + rank)
        taken = taken + jnp.sum(hit, axis=1, keepdims=True)
    slot_id = iota((SLOTS, 128), 0).astype(F32)
    pick_v[...] = (
        jnp.where(slot_id == slot_rows[0], 1.0, 0.0) + jnp.where(slot_id == slot_rows[1], 1.0, 0.0)
    ).astype(BF16)
    score = [as_column(expert_score[c : c + 1, :]) for c in range(2)]
    group = as_column(group_score[...])
    slot_columns = [as_column(line) for line in slot_rows]
    for part, size in enumerate(SIZES):
        slot_lane = (iota((ROWS, size), 1) + BOUNDS[part] * CAP).astype(F32)
        comb = jnp.zeros((ROWS, size), F32)
        for c in range(2):
            weight = group * score[c] / (score[0] + score[1])
            comb = comb + jnp.where(slot_lane == slot_columns[c], weight, 0.0)
        high, mid, _ = split3(comb)
        comb_v[part, 0:ROWS, 0:size] = mid
        comb_v[part, ROWS : 2 * ROWS, 0:size] = high

    other_rows = pl.ds(pl.multiple_of((1 - core) * ROWS, ROWS), ROWS)
    own_rows = pl.ds(pl.multiple_of(core * ROWS, ROWS), ROWS)
    swaps = [
        pltpu.make_async_remote_copy(
            src_ref=mix_v.at[p, other_rows],
            dst_ref=pair_v.at[p],
            send_sem=p_send.at[p],
            recv_sem=p_recv.at[p],
            device_id=shifted(3, 1),
            device_id_type=MESH,
        )
        for p in range(PAIRS)
    ]

    def project(mixed, whose, p):
        first = pl.multiple_of(whose * (HEADS * 128) + p * 256, 256)
        return dot(mixed, ow_v[pl.ds(first, 256), :])

    entered = [[] for _ in range(PIECES)]
    for level in (2, 1, 0):
        for piece in range(PIECES):
            p = piece // SPLIT
            await_share(level, piece)
            if piece == 0:
                lines = [line_decays(level, pair) for pair in range(PAIRS)]
            scale, total, steps = lines[p]
            enter, state = run_line(level, piece, steps)
            entered[piece].append((scale, enter))
            if level:
                upper = level - 1
                states[upper, piece, place[upper], 0:PIECE, :] = state.astype(BF16)
                if piece == 0:
                    put_decays(upper, [line[1] for line in lines])
                share(upper, piece)
            elif piece % SPLIT == SPLIT - 1:
                parts = []
                for past in entered[piece + 1 - SPLIT : piece + 1]:
                    (scale_x, enter_x), (scale_y, enter_y), (_, enter_z) = past
                    parts.append(enter_x + scale_x * (enter_y + scale_y * enter_z))
                entering = split2(jnp.concatenate(parts, axis=0))
                for h in (2 * p, 2 * p + 1):
                    mine = lane_low if h % 2 == 0 else jnp.logical_not(lane_low)
                    here = slice(h * 128, (h + 1) * 128)
                    q_h = [
                        jnp.where(mine, qd_v[i, :, p * 128 : (p + 1) * 128], none) for i in range(2)
                    ]
                    attended = att_v[:, here] + dot_split(q_h, entering, ((1,), (1,)))
                    mean = jnp.mean(attended * attended, axis=-1, keepdims=True)
                    mixed = attended * lax.rsqrt(mean + 1e-06) * gain_v[:, here]
                    mix_v[p, :, (h % 2) * 128 : (h % 2 + 1) * 128] = mixed.astype(BF16)
                swaps[p].start()
                if p == 0:
                    get_res.wait()
                    get_ow.wait()
                    acc_v[...] = res_v[...].astype(F32) + project(mix_v[p, own_rows, :], core, p)
                else:
                    acc_v[...] += project(mix_v[p, own_rows, :], core, p)
    swaps[0].wait()
    acc_v[...] += project(pair_v[0], 1 - core, 0)
    swaps[1].wait()
    summed = acc_v[...] + project(pair_v[1], 1 - core, 1)
    wide = summed.astype(BF16).astype(F32)
    acc_v[...] = wide
    mean = jnp.mean(wide * wide, axis=-1, keepdims=True)
    norm_v[...] = (wide * lax.rsqrt(mean + 1e-06) * norm_gain[...]).astype(BF16)

    def put_columns(j, block):
        for i in range(2):
            tile_v[pl.ds(2 * j + i, block.shape[0], stride=PITCH), :] = block[
                :, i * 128 : (i + 1) * 128
            ]

    def gather_tiles(dst, part):
        @pl.loop(0, SIZES[part] // 16)
        def _(g):
            for i in range(16):
                slot = g * 16 + i
                dst[BOUNDS[part] * CAP + slot] = tile_v[pl.ds(slot * PITCH, CHUNKS), :].astype(BF16)

    def to_rows(src, part):
        for g in range(SIZES[part] // 16):
            rows = src[BOUNDS[part] * CAP + g * 16 : BOUNDS[part] * CAP + (g + 1) * 16]
            nat_v[g * 16 : (g + 1) * 16, :] = rows.reshape(16, WIDTH)

    def send_part(part, src, dst, ss, rs, sign):
        @pl.loop(max(1, BOUNDS[part]), BOUNDS[part + 1])
        def _(i):
            offset = lax.rem(i * STRIDE, DEVICES)
            steps = (
                lax.div(offset, 32), lax.rem(lax.div(offset, 8), 4), lax.rem(lax.div(offset, 2), 4),
                lax.rem(offset, 2),
            )
            there = tuple(
                lax.rem(place[a] + sign * steps[a] + 4, 2 if a == 3 else 4) for a in range(4)
            )
            rows = pl.ds(i * CAP, CAP)
            pltpu.make_async_remote_copy(
                src_ref=src.at[rows],
                dst_ref=dst.at[rows],
                send_sem=ss,
                recv_sem=rs.at[part],
                device_id=there,
                device_id_type=MESH,
            ).start()

        if part == 0:
            dst[0:CAP] = src[0:CAP]

    def await_part(part, dst, rs):
        count = SIZES[part] - (CAP if part == 0 else 0)
        rows = dst.at[pl.ds(BOUNDS[part] * CAP, count)]
        pltpu.make_async_copy(rows, rows, rs.at[part]).wait()

    for part in range(PARTS):
        chosen = pick_v[BOUNDS[part] * CAP : BOUNDS[part + 1] * CAP, :]
        for j in range(WIDTH // 256):
            put_columns(j, dot(chosen, norm_v[:, j * 256 : (j + 1) * 256]))
        gather_tiles(send_v, part)
        send_part(part, send_v, recv_v, x_send, x_recv, 1)
    get_gw.wait()
    get_uw.wait()
    get_dw.wait()
    for part in range(PARTS):
        await_part(part, recv_v, x_recv)
        size = SIZES[part]
        to_rows(recv_v, part)
        for n in range(HIDDEN // 256):
            cols = slice(n * 256, (n + 1) * 256)
            gated = dot(nat_v[0:size, :], gw_v[:, cols])
            lifted = dot(nat_v[0:size, :], uw_v[:, cols])
            inner_v[0:size, cols] = (silu(gated) * lifted).astype(BF16)
        for j in range(WIDTH // 256):
            put_columns(j, dot(inner_v[0:size, :], dw_v[:, j * 256 : (j + 1) * 256]))
        gather_tiles(back_v, part)
        send_part(part, back_v, ret_v, y_send, y_recv, -1)
    for part in range(PARTS):
        await_part(part, ret_v, y_recv)
        size = SIZES[part]
        to_rows(ret_v, part)
        for j in range(WIDTH // 256):
            cols = slice(j * 256, (j + 1) * 256)
            both = dot(comb_v[part, :, 0:size], nat_v[0:size, cols])
            total = acc_v[:, cols] + (both[0:ROWS] + both[ROWS : 2 * ROWS])
            if part < PARTS - 1:
                acc_v[:, cols] = total
            else:
                out[:, cols] = total.astype(BF16)
    tiles = 9 * (128 * PAIRS + 16) // 16
    rows = send_v.at[pl.ds(0, tiles)]
    pltpu.make_async_copy(rows, rows, s_send).wait()
    for src, ss in ((send_v, x_send), (back_v, y_send)):
        rows = src.at[pl.ds(0, SLOTS - CAP)]
        pltpu.make_async_copy(rows, rows, ss).wait()


def local(
    residual, queries, key_rows, value_rows, out_gate, gate_logits, head_gain, out_weight,
    norm_gain, routes, group_score, expert_score, gate_weight, up_weight, down_weight,
):
    anywhere = pl.BlockSpec(memory_space=pl.ANY)
    vmem = pl.BlockSpec(memory_space=pltpu.VMEM)
    half = HEADS * 128
    tiles = pltpu.VMEM((SLOTS, CHUNKS, 128), BF16)
    dma = pltpu.SemaphoreType.DMA
    return pl.pallas_call(
        kernel,
        out_shape=pltpu.VMEM((ROWS, WIDTH), BF16),
        in_specs=[anywhere] * 15,
        out_specs=vmem,
        scratch_shapes=[
            pltpu.VMEM((1, 128), F32),
            pltpu.VMEM((1, WIDTH), F32),
            pltpu.VMEM((2, ROWS), I32),
            pltpu.VMEM((1, ROWS), F32),
            pltpu.VMEM((2, ROWS), F32),
            pltpu.VMEM((SEG, 256), BF16),
            pltpu.VMEM((SEG, 256), BF16),
            pltpu.VMEM((SEG, half), BF16),
            pltpu.VMEM((SEG, half), BF16),
            pltpu.VMEM((SEG, 256), BF16),
            pltpu.VMEM((ROWS, WIDTH), BF16),
            pltpu.VMEM((2 * half, WIDTH), BF16),
            pltpu.VMEM((WIDTH, HIDDEN), BF16),
            pltpu.VMEM((WIDTH, HIDDEN), BF16),
            pltpu.VMEM((HIDDEN, WIDTH), BF16),
            pltpu.VMEM((SEG, 256), F32),
            pltpu.VMEM((2, SEG, 256), BF16),
            pltpu.VMEM((SEG, half), F32),
            pltpu.VMEM((SEG, half), F32),
            pltpu.VMEM((PAIRS, SEG, 256), BF16),
            pltpu.VMEM((PAIRS, ROWS, 256), BF16),
            pltpu.VMEM((3, PIECES, 4, PIECE + 16, 128), BF16),
            pltpu.VMEM((SLOTS, ROWS), BF16),
            pltpu.VMEM((PARTS, 2 * ROWS, PART), BF16),
            pltpu.VMEM((ROWS, WIDTH), BF16),
            pltpu.VMEM((ROWS, WIDTH), F32),
            pltpu.VMEM((PART, WIDTH), BF16),
            pltpu.VMEM((PART * PITCH, 128), F32),
            tiles,
            tiles,
            pltpu.VMEM((PART, HIDDEN), BF16),
            tiles,
            tiles,
            dma((11,)), dma((4,)),
            dma, dma((3, PIECES)),
            dma((PAIRS,)), dma((PAIRS,)), dma, dma((PARTS,)), dma, dma((PARTS,)),
        ],
        compiler_params=pltpu.CompilerParams(
            collective_id=0, has_side_effects=True, vmem_limit_bytes=56 * 2**20
        ),
    )(
        residual, queries, key_rows, value_rows, out_gate, gate_logits,
        head_gain.reshape(1, 128), out_weight, norm_gain.reshape(1, WIDTH),
        routes.T, group_score.reshape(1, ROWS), expert_score.T, gate_weight, up_weight, down_weight,
    )


def solution(mesh):
    torus = Mesh(mesh.devices.reshape(4, 4, 4, mesh.shape["tp"]), AXES)
    both = P(AXES)
    in_specs = (
        P(AXES, None),
        P(SP, "tp"), P(SP, "tp"), P(SP, "tp"), P(SP, "tp"), P(SP, "tp"),
        P(), P(), P(),
        P(AXES, None), both, P(AXES, None),
        P(AXES, None, None), P(AXES, None, None), P(AXES, None, None),
    )
    return jax.shard_map(
        local, mesh=torus, in_specs=in_specs, out_specs=P(AXES, None), check_vma=False
    )
```

```python
import jax
import jax.numpy as jnp
from jax import lax
from jax.experimental import pallas as pl
from jax.experimental.pallas import tpu as pltpu
from jax.sharding import Mesh
from jax.sharding import PartitionSpec as P

AXES = ("sp_0", "sp_1", "sp_2", "tp")
SP = AXES[:3]
MESH = pl.DeviceIdType.MESH
F32, BF16, I32 = jnp.float32, jnp.bfloat16, jnp.int32

BLOCK = 64
SEG = 256
ROWS = 128
HEADS = 4
PAIRS = HEADS // 2
SPLIT = 4
PIECES = PAIRS * SPLIT
PIECE = 128 // SPLIT
WIDTH = 2048
CHUNKS = WIDTH // 128
HIDDEN = 512
DEVICES = 128
CAP = 3
SLOTS = DEVICES * CAP
BOUNDS = (0, 32, 64, 96, 128)
PARTS = len(BOUNDS) - 1
SIZES = [(BOUNDS[i + 1] - BOUNDS[i]) * CAP for i in range(PARTS)]
PART = max(SIZES)
STRIDE, UNSTRIDE = 91, 83
PITCH = CHUNKS + 1


def dot(a, b, dims=((1,), (0,))):
    return lax.dot_general(a, b, (dims, ((), ())), preferred_element_type=F32)


def split3(x):
    high = x.astype(BF16)
    rest = x - high.astype(F32)
    mid = rest.astype(BF16)
    return high, mid, (rest - mid.astype(F32)).astype(BF16)


def split2(x):
    high = x.astype(BF16)
    return high, (x - high.astype(F32)).astype(BF16)


def dot_split(a, b, dims=((1,), (0,))):
    return dot(a[0], b[0], dims) + (dot(a[0], b[1], dims) + dot(a[1], b[0], dims))


def iota(shape, dim):
    return lax.broadcasted_iota(I32, shape, dim)


def silu(x):
    return x / (1.0 + jnp.exp(-x))


def kernel(
    residual, queries, keys, values, out_gate, gate_logits, head_gain_h, out_weight, norm_gain_h,
    routes_h, group_score_h, expert_score_h, gate_weight, up_weight, down_weight,
    out,
    head_gain, norm_gain, routes, group_score, expert_score,
    q_v, k_v, v_v, og_v, gl_v, res_v, ow_v, gw_v, uw_v, dw_v,
    f_v, qd_v, att_v, gain_v, mix_v, pair_v, states, pick_v, comb_v,
    norm_v, acc_v, nat_v, tile_v, send_v, recv_v, inner_v, back_v, ret_v,
    in_sem, w_sem, s_send, s_recv, p_send, p_recv, x_send, x_recv, y_send, y_recv,
):
    place = [lax.axis_index(axis) for axis in AXES]
    core = place[3]
    me = ((place[0] * 4 + place[1]) * 4 + place[2]) * 2 + core

    def shifted(axis, step):
        there = list(place)
        size = 2 if axis == 3 else 4
        there[axis] = (place[axis] + step) % size
        return tuple(there)

    def fetch(pairs, sems, first):
        copies = [
            pltpu.make_async_copy(src, dst, sems.at[first + i]) for i, (src, dst) in enumerate(pairs)
        ]
        for copy in copies:
            copy.start()
        return copies

    get_gl, get_k, get_v, get_q, get_og, get_res = fetch(
        (
            (gate_logits, gl_v), (keys, k_v), (values, v_v), (queries, q_v), (out_gate, og_v),
            (residual, res_v),
        ),
        in_sem,
        0,
    )
    get_small = fetch(
        (
            (head_gain_h, head_gain), (norm_gain_h, norm_gain), (routes_h, routes),
            (group_score_h, group_score), (expert_score_h, expert_score),
        ),
        in_sem,
        6,
    )
    get_ow, get_gw, get_uw, get_dw = fetch(
        (
            (out_weight, ow_v), (gate_weight.at[0], gw_v), (up_weight.at[0], uw_v),
            (down_weight.at[0], dw_v),
        ),
        w_sem,
        0,
    )

    barrier = pltpu.get_barrier_semaphore()
    friends = [(axis, step) for axis in range(3) for step in (1, 2, 3)] + [(3, 1)]
    for axis, step in friends:
        pl.semaphore_signal(
            barrier, inc=1, device_id=shifted(axis, step), device_id_type=MESH
        )

    get_gl.wait()
    x = -gl_v[...].astype(F32)
    decay = -(jnp.maximum(x, 0.0) + jnp.log1p(jnp.exp(-jnp.abs(x)))) * (1.0 / 16.0)
    lower = jnp.where(iota((SEG, SEG), 0) >= iota((SEG, SEG), 1), 1.0, 0.0).astype(BF16)
    high, mid, low = split3(decay)
    f_v[...] = (dot(lower, low) + dot(lower, mid)) + dot(lower, high)

    def end_row(n):
        return f_v[pl.ds(n * BLOCK - 1, 1), :]

    lane_low = iota((1, 128), 1) < 64

    def state_after(n, p):
        rows, lanes = n * BLOCK, slice(p * 128, (p + 1) * 128)
        aged = k_v[0:rows, lanes].astype(F32) * jnp.exp(end_row(n)[:, lanes] - f_v[0:rows, lanes])
        side = []
        for i in range(2):
            v_h = v_v[0:rows, (2 * p + i) * 128 : (2 * p + i + 1) * 128]
            side.append(sum(dot(v_h, part, ((0,), (0,))) for part in split2(aged)))
        return jnp.where(lane_low, side[0], side[1])

    def put_decays(level, lines):
        part_row = iota((16, 128), 0)
        rows = jnp.zeros((16, 128), F32)
        for p in range(PAIRS):
            for i, part in enumerate(split3(lines[p])):
                rows = jnp.where(part_row == 3 * p + i, part.astype(F32), rows)
        states[level, 0, place[level], PIECE : PIECE + 16, :] = rows.astype(BF16)

    def piece_rows(piece):
        return pl.ds(0, PIECE + 16 if piece == 0 else PIECE)

    def share(level, piece):
        here = place[level]
        for step in (2, 1, 3):
            pltpu.make_async_remote_copy(
                src_ref=states.at[level, piece, here, piece_rows(piece)],
                dst_ref=states.at[level, piece, here, piece_rows(piece)],
                send_sem=s_send,
                recv_sem=s_recv.at[level, piece],
                device_id=shifted(level, step),
                device_id_type=MESH,
            ).start()

    def await_share(level, piece):
        three = states.at[level, piece, pl.ds(0, 3), piece_rows(piece)]
        pltpu.make_async_copy(three, three, s_recv.at[level, piece]).wait()

    def line_decays(level, p):
        here = place[level]
        total = jnp.zeros((1, 128), F32)
        before = total
        steps = []
        for j in range(4):
            before = jnp.where(here == j, total, before)
            parts = states[level, 0, j, PIECE : PIECE + 16, :].astype(F32)
            step = (parts[3 * p + 2 : 3 * p + 3] + parts[3 * p + 1 : 3 * p + 2]) + parts[3 * p : 3 * p + 1]
            steps.append(jnp.exp(step))
            total = total + step
        return jnp.exp(before), total, steps

    def run_line(level, piece, steps):
        here = place[level]
        state = jnp.zeros((PIECE, 128), F32)
        enter = state
        for j in range(4):
            enter = jnp.where(here == j, state, enter)
            state = state * steps[j] + states[level, piece, j, 0:PIECE, :].astype(F32)
        return enter, state

    get_k.wait()
    get_v.wait()
    whole = end_row(SEG // BLOCK)
    put_decays(2, [whole[:, p * 128 : (p + 1) * 128] for p in range(PAIRS)])
    for p in range(PAIRS):
        local_end = state_after(SEG // BLOCK, p).astype(BF16)
        for i in range(SPLIT):
            states[2, p * SPLIT + i, place[2], 0:PIECE, :] = local_end[i * PIECE : (i + 1) * PIECE]
        if p == 0:
            pl.semaphore_wait(barrier, len(friends))
        for i in range(SPLIT):
            share(2, p * SPLIT + i)
    get_q.wait()
    scale = 64.0 ** (-0.5)
    block_row = iota((SEG, 1), 0) // BLOCK
    f = f_v[...]
    start = jnp.zeros((SEG, 256), F32)
    for n in range(1, SEG // BLOCK):
        start = jnp.where(block_row == n, end_row(n), start)
    running = f - start
    q = q_v[...].astype(F32) * scale
    for i, part in enumerate(split2(q * jnp.exp(f))):
        qd_v[i] = part
    q_scaled = split2(q * jnp.exp(running))
    k_inverse = split2(k_v[...].astype(F32) * jnp.exp(-running))
    row, col = iota((SEG, SEG), 0), iota((SEG, SEG), 1)
    causal = (row >= col) & (row // BLOCK == col // BLOCK)
    none = jnp.zeros((), BF16)
    local_states = [None] + [
        [split2(state_after(n, p)) for p in range(PAIRS)] for n in range(1, SEG // BLOCK)
    ]
    for h in range(HEADS):
        p = h // 2
        mine = lane_low if h % 2 == 0 else jnp.logical_not(lane_low)
        lanes = slice(p * 128, (p + 1) * 128)
        q_h = [jnp.where(mine, part[:, lanes], none) for part in q_scaled]
        k_h = [jnp.where(mine, part[:, lanes], none) for part in k_inverse]
        scores = jnp.where(causal, dot_split(q_h, k_h, ((1,), (1,))), 0.0)
        here = slice(h * 128, (h + 1) * 128)
        att_v[:, here] = sum(dot(part, v_v[:, here]) for part in split2(scores))
        for n in range(1, SEG // BLOCK):
            rows = slice(n * BLOCK, (n + 1) * BLOCK)
            q_n = [part[rows] for part in q_h]
            att_v[rows, here] += dot_split(q_n, local_states[n][p], ((1,), (1,)))
    get_og.wait()
    for copy in get_small:
        copy.wait()
    for h in range(HEADS):
        here = slice(h * 128, (h + 1) * 128)
        gain_v[:, here] = silu(og_v[:, here].astype(F32)) * head_gain[...]

    diagonal = iota((128, 128), 0) == iota((128, 128), 1)

    def as_column(line):
        return jnp.sum(jnp.where(diagonal, line, 0.0), axis=1, keepdims=True)

    expert_id = iota((128, 128), 0)
    earlier = jnp.where(iota((128, 128), 0) < iota((128, 128), 1), 1.0, 0.0).astype(BF16)
    taken = jnp.zeros((128, 1), F32)
    slot_rows = []
    for c in range(2):
        line = routes[c : c + 1, :]
        hit = jnp.where(expert_id == line, 1.0, 0.0)
        count = dot(hit.astype(BF16), earlier) + taken
        rank = jnp.sum(hit * count, axis=0, keepdims=True)
        offset = jnp.zeros_like(line)
        for a, unit in enumerate((32, 8, 2, 1)):
            size = 2 if a == 3 else 4
            offset = offset + unit * ((line // unit % size - place[a] + size) % size)
        step = offset * UNSTRIDE % DEVICES
        slot_rows.append((step * CAP).astype(F32) + rank)
        taken = taken + jnp.sum(hit, axis=1, keepdims=True)
    slot_id = iota((SLOTS, 128), 0).astype(F32)
    pick_v[...] = (
        jnp.where(slot_id == slot_rows[0], 1.0, 0.0) + jnp.where(slot_id == slot_rows[1], 1.0, 0.0)
    ).astype(BF16)
    score = [as_column(expert_score[c : c + 1, :]) for c in range(2)]
    group = as_column(group_score[...])
    slot_columns = [as_column(line) for line in slot_rows]
    for part, size in enumerate(SIZES):
        slot_lane = (iota((ROWS, size), 1) + BOUNDS[part] * CAP).astype(F32)
        comb = jnp.zeros((ROWS, size), F32)
        for c in range(2):
            weight = group * score[c] / (score[0] + score[1])
            comb = comb + jnp.where(slot_lane == slot_columns[c], weight, 0.0)
        high, mid, _ = split3(comb)
        comb_v[part, 0:ROWS, 0:size] = mid
        comb_v[part, ROWS : 2 * ROWS, 0:size] = high

    other_rows = pl.ds(pl.multiple_of((1 - core) * ROWS, ROWS), ROWS)
    own_rows = pl.ds(pl.multiple_of(core * ROWS, ROWS), ROWS)
    swaps = [
        pltpu.make_async_remote_copy(
            src_ref=mix_v.at[p, other_rows],
            dst_ref=pair_v.at[p],
            send_sem=p_send.at[p],
            recv_sem=p_recv.at[p],
            device_id=shifted(3, 1),
            device_id_type=MESH,
        )
        for p in range(PAIRS)
    ]

    def project(mixed, whose, p):
        first = pl.multiple_of(whose * (HEADS * 128) + p * 256, 256)
        return dot(mixed, ow_v[pl.ds(first, 256), :])

    entered = [[] for _ in range(PIECES)]
    for level in (2, 1, 0):
        for piece in range(PIECES):
            p = piece // SPLIT
            await_share(level, piece)
            if piece == 0:
                lines = [line_decays(level, pair) for pair in range(PAIRS)]
            scale, total, steps = lines[p]
            enter, state = run_line(level, piece, steps)
            entered[piece].append((scale, enter))
            if level:
                upper = level - 1
                states[upper, piece, place[upper], 0:PIECE, :] = state.astype(BF16)
                if piece == 0:
                    put_decays(upper, [line[1] for line in lines])
                share(upper, piece)
            elif piece % SPLIT == SPLIT - 1:
                parts = []
                for past in entered[piece + 1 - SPLIT : piece + 1]:
                    (scale_x, enter_x), (scale_y, enter_y), (_, enter_z) = past
                    parts.append(enter_x + scale_x * (enter_y + scale_y * enter_z))
                entering = split2(jnp.concatenate(parts, axis=0))
                for h in (2 * p, 2 * p + 1):
                    mine = lane_low if h % 2 == 0 else jnp.logical_not(lane_low)
                    here = slice(h * 128, (h + 1) * 128)
                    q_h = [
                        jnp.where(mine, qd_v[i, :, p * 128 : (p + 1) * 128], none) for i in range(2)
                    ]
                    attended = att_v[:, here] + dot_split(q_h, entering, ((1,), (1,)))
                    mean = jnp.mean(attended * attended, axis=-1, keepdims=True)
                    mixed = attended * lax.rsqrt(mean + 1e-06) * gain_v[:, here]
                    mix_v[p, :, (h % 2) * 128 : (h % 2 + 1) * 128] = mixed.astype(BF16)
                swaps[p].start()
                if p == 0:
                    get_res.wait()
                    get_ow.wait()
                    acc_v[...] = res_v[...].astype(F32) + project(mix_v[p, own_rows, :], core, p)
                else:
                    acc_v[...] += project(mix_v[p, own_rows, :], core, p)
    swaps[0].wait()
    acc_v[...] += project(pair_v[0], 1 - core, 0)
    swaps[1].wait()
    summed = acc_v[...] + project(pair_v[1], 1 - core, 1)
    merged = summed.astype(BF16)
    norm_v[...] = merged

    def put_columns(j, block):
        for i in range(2):
            tile_v[pl.ds(2 * j + i, block.shape[0], stride=PITCH), :] = block[
                :, i * 128 : (i + 1) * 128
            ]

    def gather_tiles(dst, part):
        @pl.loop(0, SIZES[part] // 16)
        def _(g):
            for i in range(16):
                slot = g * 16 + i
                dst[BOUNDS[part] * CAP + slot] = tile_v[pl.ds(slot * PITCH, CHUNKS), :].astype(BF16)

    def to_rows(src, part):
        for g in range(SIZES[part] // 16):
            rows = src[BOUNDS[part] * CAP + g * 16 : BOUNDS[part] * CAP + (g + 1) * 16]
            nat_v[g * 16 : (g + 1) * 16, :] = rows.reshape(16, WIDTH)

    def send_part(part, src, dst, ss, rs, sign):
        @pl.loop(max(1, BOUNDS[part]), BOUNDS[part + 1])
        def _(i):
            offset = lax.rem(i * STRIDE, DEVICES)
            steps = (
                lax.div(offset, 32), lax.rem(lax.div(offset, 8), 4), lax.rem(lax.div(offset, 2), 4),
                lax.rem(offset, 2),
            )
            there = tuple(
                lax.rem(place[a] + sign * steps[a] + 4, 2 if a == 3 else 4) for a in range(4)
            )
            rows = pl.ds(i * CAP, CAP)
            pltpu.make_async_remote_copy(
                src_ref=src.at[rows],
                dst_ref=dst.at[rows],
                send_sem=ss,
                recv_sem=rs.at[part],
                device_id=there,
                device_id_type=MESH,
            ).start()

        if part == 0:
            dst[0:CAP] = src[0:CAP]

    def await_part(part, dst, rs):
        count = SIZES[part] - (CAP if part == 0 else 0)
        rows = dst.at[pl.ds(BOUNDS[part] * CAP, count)]
        pltpu.make_async_copy(rows, rows, rs.at[part]).wait()

    for part in range(PARTS):
        chosen = pick_v[BOUNDS[part] * CAP : BOUNDS[part + 1] * CAP, :]
        for j in range(WIDTH // 256):
            put_columns(j, dot(chosen, norm_v[:, j * 256 : (j + 1) * 256]))
        gather_tiles(send_v, part)
        send_part(part, send_v, recv_v, x_send, x_recv, 1)
    acc_v[...] = norm_v[...].astype(F32)
    get_gw.wait()
    get_uw.wait()
    get_dw.wait()
    for part in range(PARTS):
        await_part(part, recv_v, x_recv)
        size = SIZES[part]
        to_rows(recv_v, part)
        wide = nat_v[0:size, :].astype(F32)
        mean = jnp.mean(wide * wide, axis=-1, keepdims=True)
        nat_v[0:size, :] = (wide * lax.rsqrt(mean + 1e-06) * norm_gain[...]).astype(BF16)
        for n in range(HIDDEN // 256):
            cols = slice(n * 256, (n + 1) * 256)
            gated = dot(nat_v[0:size, :], gw_v[:, cols])
            lifted = dot(nat_v[0:size, :], uw_v[:, cols])
            inner_v[0:size, cols] = (silu(gated) * lifted).astype(BF16)
        for j in range(WIDTH // 256):
            put_columns(j, dot(inner_v[0:size, :], dw_v[:, j * 256 : (j + 1) * 256]))
        gather_tiles(back_v, part)
        send_part(part, back_v, ret_v, y_send, y_recv, -1)
    for part in range(PARTS):
        await_part(part, ret_v, y_recv)
        size = SIZES[part]
        to_rows(ret_v, part)
        for j in range(WIDTH // 256):
            cols = slice(j * 256, (j + 1) * 256)
            both = dot(comb_v[part, :, 0:size], nat_v[0:size, cols])
            total = acc_v[:, cols] + (both[0:ROWS] + both[ROWS : 2 * ROWS])
            if part < PARTS - 1:
                acc_v[:, cols] = total
            else:
                out[:, cols] = total.astype(BF16)
    tiles = 9 * (128 * PAIRS + 16) // 16
    rows = send_v.at[pl.ds(0, tiles)]
    pltpu.make_async_copy(rows, rows, s_send).wait()
    for src, ss in ((send_v, x_send), (back_v, y_send)):
        rows = src.at[pl.ds(0, SLOTS - CAP)]
        pltpu.make_async_copy(rows, rows, ss).wait()


def local(
    residual, queries, key_rows, value_rows, out_gate, gate_logits, head_gain, out_weight,
    norm_gain, routes, group_score, expert_score, gate_weight, up_weight, down_weight,
):
    anywhere = pl.BlockSpec(memory_space=pl.ANY)
    vmem = pl.BlockSpec(memory_space=pltpu.VMEM)
    half = HEADS * 128
    tiles = pltpu.VMEM((SLOTS, CHUNKS, 128), BF16)
    dma = pltpu.SemaphoreType.DMA
    return pl.pallas_call(
        kernel,
        out_shape=pltpu.VMEM((ROWS, WIDTH), BF16),
        in_specs=[anywhere] * 15,
        out_specs=vmem,
        scratch_shapes=[
            pltpu.VMEM((1, 128), F32),
            pltpu.VMEM((1, WIDTH), F32),
            pltpu.VMEM((2, ROWS), I32),
            pltpu.VMEM((1, ROWS), F32),
            pltpu.VMEM((2, ROWS), F32),
            pltpu.VMEM((SEG, 256), BF16),
            pltpu.VMEM((SEG, 256), BF16),
            pltpu.VMEM((SEG, half), BF16),
            pltpu.VMEM((SEG, half), BF16),
            pltpu.VMEM((SEG, 256), BF16),
            pltpu.VMEM((ROWS, WIDTH), BF16),
            pltpu.VMEM((2 * half, WIDTH), BF16),
            pltpu.VMEM((WIDTH, HIDDEN), BF16),
            pltpu.VMEM((WIDTH, HIDDEN), BF16),
            pltpu.VMEM((HIDDEN, WIDTH), BF16),
            pltpu.VMEM((SEG, 256), F32),
            pltpu.VMEM((2, SEG, 256), BF16),
            pltpu.VMEM((SEG, half), F32),
            pltpu.VMEM((SEG, half), F32),
            pltpu.VMEM((PAIRS, SEG, 256), BF16),
            pltpu.VMEM((PAIRS, ROWS, 256), BF16),
            pltpu.VMEM((3, PIECES, 4, PIECE + 16, 128), BF16),
            pltpu.VMEM((SLOTS, ROWS), BF16),
            pltpu.VMEM((PARTS, 2 * ROWS, PART), BF16),
            pltpu.VMEM((ROWS, WIDTH), BF16),
            pltpu.VMEM((ROWS, WIDTH), F32),
            pltpu.VMEM((PART, WIDTH), BF16),
            pltpu.VMEM(((PART + 2) * PITCH, 128), F32),
            tiles,
            tiles,
            pltpu.VMEM((PART, HIDDEN), BF16),
            tiles,
            tiles,
            dma((11,)), dma((4,)),
            dma, dma((3, PIECES)),
            dma((PAIRS,)), dma((PAIRS,)), dma, dma((PARTS,)), dma, dma((PARTS,)),
        ],
        compiler_params=pltpu.CompilerParams(
            collective_id=0, has_side_effects=True, vmem_limit_bytes=56 * 2**20
        ),
    )(
        residual, queries, key_rows, value_rows, out_gate, gate_logits,
        head_gain.reshape(1, 128), out_weight, norm_gain.reshape(1, WIDTH),
        routes.T, group_score.reshape(1, ROWS), expert_score.T, gate_weight, up_weight, down_weight,
    )


def solution(mesh):
    torus = Mesh(mesh.devices.reshape(4, 4, 4, mesh.shape["tp"]), AXES)
    both = P(AXES)
    in_specs = (
        P(AXES, None),
        P(SP, "tp"), P(SP, "tp"), P(SP, "tp"), P(SP, "tp"), P(SP, "tp"),
        P(), P(), P(),
        P(AXES, None), both, P(AXES, None),
        P(AXES, None, None), P(AXES, None, None), P(AXES, None, None),
    )
    return jax.shard_map(
        local, mesh=torus, in_specs=in_specs, out_specs=P(AXES, None), check_vma=False
    )
```

```python
import jax
import jax.numpy as jnp
from jax import lax
from jax.experimental import pallas as pl
from jax.experimental.pallas import tpu as pltpu
from jax.sharding import Mesh
from jax.sharding import PartitionSpec as P

AXES = ("sp_0", "sp_1", "sp_2", "tp")
SP = AXES[:3]
MESH = pl.DeviceIdType.MESH
F32, BF16, I32 = jnp.float32, jnp.bfloat16, jnp.int32

BLOCK = 64
SEG = 256
ROWS = 128
HEADS = 4
PAIRS = HEADS // 2
SPLIT = 4
PIECES = PAIRS * SPLIT
PIECE = 128 // SPLIT
WIDTH = 2048
CHUNKS = WIDTH // 128
HIDDEN = 512
DEVICES = 128
CAP = 3
SLOTS = DEVICES * CAP
BOUNDS = (0, 48, 96, 128)
PARTS = len(BOUNDS) - 1
SIZES = [(BOUNDS[i + 1] - BOUNDS[i]) * CAP for i in range(PARTS)]
PART = max(SIZES)
STRIDE, UNSTRIDE = 91, 83
PITCH = CHUNKS + 1


def dot(a, b, dims=((1,), (0,))):
    return lax.dot_general(a, b, (dims, ((), ())), preferred_element_type=F32)


def split3(x):
    high = x.astype(BF16)
    rest = x - high.astype(F32)
    mid = rest.astype(BF16)
    return high, mid, (rest - mid.astype(F32)).astype(BF16)


def split2(x):
    high = x.astype(BF16)
    return high, (x - high.astype(F32)).astype(BF16)


def dot_split(a, b, dims=((1,), (0,))):
    return dot(a[0], b[0], dims) + (dot(a[0], b[1], dims) + dot(a[1], b[0], dims))


def iota(shape, dim):
    return lax.broadcasted_iota(I32, shape, dim)


def silu(x):
    return x / (1.0 + jnp.exp(-x))


def kernel(
    residual, queries, keys, values, out_gate, gate_logits, head_gain_h, out_weight, norm_gain_h,
    routes_h, group_score_h, expert_score_h, gate_weight, up_weight, down_weight,
    out,
    head_gain, norm_gain, routes, group_score, expert_score,
    q_v, k_v, v_v, og_v, gl_v, res_v, ow_v, gw_v, uw_v, dw_v,
    f_v, qd_v, att_v, gain_v, mix_v, pair_v, states, pick_v, comb_v,
    norm_v, acc_v, nat_v, tile_v, send_v, recv_v, inner_v, back_v, ret_v,
    in_sem, w_sem, s_send, s_recv, p_send, p_recv, x_send, x_recv, y_send, y_recv,
):
    place = [lax.axis_index(axis) for axis in AXES]
    core = place[3]
    me = ((place[0] * 4 + place[1]) * 4 + place[2]) * 2 + core

    def shifted(axis, step):
        there = list(place)
        size = 2 if axis == 3 else 4
        there[axis] = (place[axis] + step) % size
        return tuple(there)

    def fetch(pairs, sems, first):
        copies = [
            pltpu.make_async_copy(src, dst, sems.at[first + i]) for i, (src, dst) in enumerate(pairs)
        ]
        for copy in copies:
            copy.start()
        return copies

    get_gl, get_k, get_v, get_q, get_og, get_res = fetch(
        (
            (gate_logits, gl_v), (keys, k_v), (values, v_v), (queries, q_v), (out_gate, og_v),
            (residual, res_v),
        ),
        in_sem,
        0,
    )
    get_small = fetch(
        (
            (head_gain_h, head_gain), (norm_gain_h, norm_gain), (routes_h, routes),
            (group_score_h, group_score), (expert_score_h, expert_score),
        ),
        in_sem,
        6,
    )
    get_ow, get_gw, get_uw, get_dw = fetch(
        (
            (out_weight, ow_v), (gate_weight.at[0], gw_v), (up_weight.at[0], uw_v),
            (down_weight.at[0], dw_v),
        ),
        w_sem,
        0,
    )

    barrier = pltpu.get_barrier_semaphore()
    friends = [(axis, step) for axis in range(3) for step in (1, 2, 3)] + [(3, 1)]
    for axis, step in friends:
        pl.semaphore_signal(
            barrier, inc=1, device_id=shifted(axis, step), device_id_type=MESH
        )

    get_gl.wait()
    x = -gl_v[...].astype(F32)
    decay = -(jnp.maximum(x, 0.0) + jnp.log1p(jnp.exp(-jnp.abs(x)))) * (1.0 / 16.0)
    lower = jnp.where(iota((SEG, SEG), 0) >= iota((SEG, SEG), 1), 1.0, 0.0).astype(BF16)
    high, mid, low = split3(decay)
    f_v[...] = (dot(lower, low) + dot(lower, mid)) + dot(lower, high)

    def end_row(n):
        return f_v[pl.ds(n * BLOCK - 1, 1), :]

    lane_low = iota((1, 128), 1) < 64

    def state_after(n, p):
        rows, lanes = n * BLOCK, slice(p * 128, (p + 1) * 128)
        aged = k_v[0:rows, lanes].astype(F32) * jnp.exp(end_row(n)[:, lanes] - f_v[0:rows, lanes])
        side = []
        for i in range(2):
            v_h = v_v[0:rows, (2 * p + i) * 128 : (2 * p + i + 1) * 128]
            side.append(sum(dot(v_h, part, ((0,), (0,))) for part in split2(aged)))
        return jnp.where(lane_low, side[0], side[1])

    def put_decays(level, lines):
        part_row = iota((16, 128), 0)
        rows = jnp.zeros((16, 128), F32)
        for p in range(PAIRS):
            for i, part in enumerate(split3(lines[p])):
                rows = jnp.where(part_row == 3 * p + i, part.astype(F32), rows)
        states[level, 0, place[level], PIECE : PIECE + 16, :] = rows.astype(BF16)

    def piece_rows(piece):
        return pl.ds(0, PIECE + 16 if piece == 0 else PIECE)

    def share(level, piece):
        here = place[level]
        for step in (2, 1, 3):
            pltpu.make_async_remote_copy(
                src_ref=states.at[level, piece, here, piece_rows(piece)],
                dst_ref=states.at[level, piece, here, piece_rows(piece)],
                send_sem=s_send,
                recv_sem=s_recv.at[level, piece],
                device_id=shifted(level, step),
                device_id_type=MESH,
            ).start()

    def await_share(level, piece):
        three = states.at[level, piece, pl.ds(0, 3), piece_rows(piece)]
        pltpu.make_async_copy(three, three, s_recv.at[level, piece]).wait()

    def line_decays(level, p):
        here = place[level]
        total = jnp.zeros((1, 128), F32)
        before = total
        steps = []
        for j in range(4):
            before = jnp.where(here == j, total, before)
            parts = states[level, 0, j, PIECE : PIECE + 16, :].astype(F32)
            step = (parts[3 * p + 2 : 3 * p + 3] + parts[3 * p + 1 : 3 * p + 2]) + parts[3 * p : 3 * p + 1]
            steps.append(jnp.exp(step))
            total = total + step
        return jnp.exp(before), total, steps

    def run_line(level, piece, steps):
        here = place[level]
        state = jnp.zeros((PIECE, 128), F32)
        enter = state
        for j in range(4):
            enter = jnp.where(here == j, state, enter)
            state = state * steps[j] + states[level, piece, j, 0:PIECE, :].astype(F32)
        return enter, state

    get_k.wait()
    get_v.wait()
    whole = end_row(SEG // BLOCK)
    put_decays(2, [whole[:, p * 128 : (p + 1) * 128] for p in range(PAIRS)])
    for p in range(PAIRS):
        local_end = state_after(SEG // BLOCK, p).astype(BF16)
        for i in range(SPLIT):
            states[2, p * SPLIT + i, place[2], 0:PIECE, :] = local_end[i * PIECE : (i + 1) * PIECE]
        if p == 0:
            pl.semaphore_wait(barrier, len(friends))
        for i in range(SPLIT):
            share(2, p * SPLIT + i)
    get_q.wait()
    scale = 64.0 ** (-0.5)
    block_row = iota((SEG, 1), 0) // BLOCK
    f = f_v[...]
    start = jnp.zeros((SEG, 256), F32)
    for n in range(1, SEG // BLOCK):
        start = jnp.where(block_row == n, end_row(n), start)
    running = f - start
    q = q_v[...].astype(F32) * scale
    for i, part in enumerate(split2(q * jnp.exp(f))):
        qd_v[i] = part
    q_scaled = split2(q * jnp.exp(running))
    k_inverse = split2(k_v[...].astype(F32) * jnp.exp(-running))
    row, col = iota((SEG, SEG), 0), iota((SEG, SEG), 1)
    causal = (row >= col) & (row // BLOCK == col // BLOCK)
    none = jnp.zeros((), BF16)
    local_states = [None] + [
        [split2(state_after(n, p)) for p in range(PAIRS)] for n in range(1, SEG // BLOCK)
    ]
    for h in range(HEADS):
        p = h // 2
        mine = lane_low if h % 2 == 0 else jnp.logical_not(lane_low)
        lanes = slice(p * 128, (p + 1) * 128)
        q_h = [jnp.where(mine, part[:, lanes], none) for part in q_scaled]
        k_h = [jnp.where(mine, part[:, lanes], none) for part in k_inverse]
        scores = jnp.where(causal, dot_split(q_h, k_h, ((1,), (1,))), 0.0)
        here = slice(h * 128, (h + 1) * 128)
        att_v[:, here] = sum(dot(part, v_v[:, here]) for part in split2(scores))
        for n in range(1, SEG // BLOCK):
            rows = slice(n * BLOCK, (n + 1) * BLOCK)
            q_n = [part[rows] for part in q_h]
            att_v[rows, here] += dot_split(q_n, local_states[n][p], ((1,), (1,)))
    get_og.wait()
    for copy in get_small:
        copy.wait()
    for h in range(HEADS):
        here = slice(h * 128, (h + 1) * 128)
        gain_v[:, here] = silu(og_v[:, here].astype(F32)) * head_gain[...]

    diagonal = iota((128, 128), 0) == iota((128, 128), 1)

    def as_column(line):
        return jnp.sum(jnp.where(diagonal, line, 0.0), axis=1, keepdims=True)

    expert_id = iota((128, 128), 0)
    earlier = jnp.where(iota((128, 128), 0) < iota((128, 128), 1), 1.0, 0.0).astype(BF16)
    taken = jnp.zeros((128, 1), F32)
    slot_rows = []
    for c in range(2):
        line = routes[c : c + 1, :]
        hit = jnp.where(expert_id == line, 1.0, 0.0)
        count = dot(hit.astype(BF16), earlier) + taken
        rank = jnp.sum(hit * count, axis=0, keepdims=True)
        offset = jnp.zeros_like(line)
        for a, unit in enumerate((32, 8, 2, 1)):
            size = 2 if a == 3 else 4
            offset = offset + unit * ((line // unit % size - place[a] + size) % size)
        step = offset * UNSTRIDE % DEVICES
        slot_rows.append((step * CAP).astype(F32) + rank)
        taken = taken + jnp.sum(hit, axis=1, keepdims=True)
    slot_id = iota((SLOTS, 128), 0).astype(F32)
    pick_v[...] = (
        jnp.where(slot_id == slot_rows[0], 1.0, 0.0) + jnp.where(slot_id == slot_rows[1], 1.0, 0.0)
    ).astype(BF16)
    score = [as_column(expert_score[c : c + 1, :]) for c in range(2)]
    group = as_column(group_score[...])
    slot_columns = [as_column(line) for line in slot_rows]
    for part, size in enumerate(SIZES):
        slot_lane = (iota((ROWS, size), 1) + BOUNDS[part] * CAP).astype(F32)
        comb = jnp.zeros((ROWS, size), F32)
        for c in range(2):
            weight = group * score[c] / (score[0] + score[1])
            comb = comb + jnp.where(slot_lane == slot_columns[c], weight, 0.0)
        high, mid, _ = split3(comb)
        comb_v[part, 0:ROWS, 0:size] = mid
        comb_v[part, ROWS : 2 * ROWS, 0:size] = high

    other_rows = pl.ds(pl.multiple_of((1 - core) * ROWS, ROWS), ROWS)
    own_rows = pl.ds(pl.multiple_of(core * ROWS, ROWS), ROWS)
    swaps = [
        pltpu.make_async_remote_copy(
            src_ref=mix_v.at[p, other_rows],
            dst_ref=pair_v.at[p],
            send_sem=p_send.at[p],
            recv_sem=p_recv.at[p],
            device_id=shifted(3, 1),
            device_id_type=MESH,
        )
        for p in range(PAIRS)
    ]

    def project(mixed, whose, p):
        first = pl.multiple_of(whose * (HEADS * 128) + p * 256, 256)
        return dot(mixed, ow_v[pl.ds(first, 256), :])

    entered = [[] for _ in range(PIECES)]
    for level in (2, 1, 0):
        for piece in range(PIECES):
            p = piece // SPLIT
            await_share(level, piece)
            if piece == 0:
                lines = [line_decays(level, pair) for pair in range(PAIRS)]
            scale, total, steps = lines[p]
            enter, state = run_line(level, piece, steps)
            entered[piece].append((scale, enter))
            if level:
                upper = level - 1
                states[upper, piece, place[upper], 0:PIECE, :] = state.astype(BF16)
                if piece == 0:
                    put_decays(upper, [line[1] for line in lines])
                share(upper, piece)
            elif piece % SPLIT == SPLIT - 1:
                parts = []
                for past in entered[piece + 1 - SPLIT : piece + 1]:
                    (scale_x, enter_x), (scale_y, enter_y), (_, enter_z) = past
                    parts.append(enter_x + scale_x * (enter_y + scale_y * enter_z))
                entering = split2(jnp.concatenate(parts, axis=0))
                for h in (2 * p, 2 * p + 1):
                    mine = lane_low if h % 2 == 0 else jnp.logical_not(lane_low)
                    here = slice(h * 128, (h + 1) * 128)
                    q_h = [
                        jnp.where(mine, qd_v[i, :, p * 128 : (p + 1) * 128], none) for i in range(2)
                    ]
                    attended = att_v[:, here] + dot_split(q_h, entering, ((1,), (1,)))
                    mean = jnp.mean(attended * attended, axis=-1, keepdims=True)
                    mixed = attended * lax.rsqrt(mean + 1e-06) * gain_v[:, here]
                    mix_v[p, :, (h % 2) * 128 : (h % 2 + 1) * 128] = mixed.astype(BF16)
                swaps[p].start()
                if p == 0:
                    get_res.wait()
                    get_ow.wait()
                    acc_v[...] = res_v[...].astype(F32) + project(mix_v[p, own_rows, :], core, p)
                else:
                    acc_v[...] += project(mix_v[p, own_rows, :], core, p)
    swaps[0].wait()
    acc_v[...] += project(pair_v[0], 1 - core, 0)
    swaps[1].wait()
    summed = acc_v[...] + project(pair_v[1], 1 - core, 1)
    merged = summed.astype(BF16)
    norm_v[...] = merged

    def put_columns(j, block):
        for i in range(2):
            tile_v[pl.ds(2 * j + i, block.shape[0], stride=PITCH), :] = block[
                :, i * 128 : (i + 1) * 128
            ]

    def gather_tiles(dst, part):
        @pl.loop(0, SIZES[part] // 16)
        def _(g):
            for i in range(16):
                slot = g * 16 + i
                dst[BOUNDS[part] * CAP + slot] = tile_v[pl.ds(slot * PITCH, CHUNKS), :].astype(BF16)

    def to_rows(src, part):
        for g in range(SIZES[part] // 16):
            rows = src[BOUNDS[part] * CAP + g * 16 : BOUNDS[part] * CAP + (g + 1) * 16]
            nat_v[g * 16 : (g + 1) * 16, :] = rows.reshape(16, WIDTH)

    def send_part(part, src, dst, ss, rs, sign):
        @pl.loop(max(1, BOUNDS[part]), BOUNDS[part + 1])
        def _(i):
            offset = lax.rem(i * STRIDE, DEVICES)
            steps = (
                lax.div(offset, 32), lax.rem(lax.div(offset, 8), 4), lax.rem(lax.div(offset, 2), 4),
                lax.rem(offset, 2),
            )
            there = tuple(
                lax.rem(place[a] + sign * steps[a] + 4, 2 if a == 3 else 4) for a in range(4)
            )
            rows = pl.ds(i * CAP, CAP)
            pltpu.make_async_remote_copy(
                src_ref=src.at[rows],
                dst_ref=dst.at[rows],
                send_sem=ss,
                recv_sem=rs.at[part],
                device_id=there,
                device_id_type=MESH,
            ).start()

        if part == 0:
            dst[0:CAP] = src[0:CAP]

    def await_part(part, dst, rs):
        count = SIZES[part] - (CAP if part == 0 else 0)
        rows = dst.at[pl.ds(BOUNDS[part] * CAP, count)]
        pltpu.make_async_copy(rows, rows, rs.at[part]).wait()

    for part in range(PARTS):
        chosen = pick_v[BOUNDS[part] * CAP : BOUNDS[part + 1] * CAP, :]
        for j in range(WIDTH // 256):
            put_columns(j, dot(chosen, norm_v[:, j * 256 : (j + 1) * 256]))
        gather_tiles(send_v, part)
        send_part(part, send_v, recv_v, x_send, x_recv, 1)
    acc_v[...] = norm_v[...].astype(F32)
    get_gw.wait()
    get_uw.wait()
    get_dw.wait()
    for part in range(PARTS):
        await_part(part, recv_v, x_recv)
        size = SIZES[part]
        to_rows(recv_v, part)
        wide = nat_v[0:size, :].astype(F32)
        mean = jnp.mean(wide * wide, axis=-1, keepdims=True)
        nat_v[0:size, :] = (wide * lax.rsqrt(mean + 1e-06) * norm_gain[...]).astype(BF16)
        for n in range(HIDDEN // 256):
            cols = slice(n * 256, (n + 1) * 256)
            gated = dot(nat_v[0:size, :], gw_v[:, cols])
            lifted = dot(nat_v[0:size, :], uw_v[:, cols])
            inner_v[0:size, cols] = (silu(gated) * lifted).astype(BF16)
        for j in range(WIDTH // 256):
            put_columns(j, dot(inner_v[0:size, :], dw_v[:, j * 256 : (j + 1) * 256]))
        gather_tiles(back_v, part)
        send_part(part, back_v, ret_v, y_send, y_recv, -1)
    for part in range(PARTS):
        await_part(part, ret_v, y_recv)
        size = SIZES[part]
        to_rows(ret_v, part)
        for j in range(WIDTH // 256):
            cols = slice(j * 256, (j + 1) * 256)
            both = dot(comb_v[part, :, 0:size], nat_v[0:size, cols])
            total = acc_v[:, cols] + (both[0:ROWS] + both[ROWS : 2 * ROWS])
            if part < PARTS - 1:
                acc_v[:, cols] = total
            else:
                out[:, cols] = total.astype(BF16)
    tiles = 9 * (128 * PAIRS + 16) // 16
    rows = send_v.at[pl.ds(0, tiles)]
    pltpu.make_async_copy(rows, rows, s_send).wait()
    for src, ss in ((send_v, x_send), (back_v, y_send)):
        rows = src.at[pl.ds(0, SLOTS - CAP)]
        pltpu.make_async_copy(rows, rows, ss).wait()


def local(
    residual, queries, key_rows, value_rows, out_gate, gate_logits, head_gain, out_weight,
    norm_gain, routes, group_score, expert_score, gate_weight, up_weight, down_weight,
):
    anywhere = pl.BlockSpec(memory_space=pl.ANY)
    vmem = pl.BlockSpec(memory_space=pltpu.VMEM)
    half = HEADS * 128
    tiles = pltpu.VMEM((SLOTS, CHUNKS, 128), BF16)
    dma = pltpu.SemaphoreType.DMA
    return pl.pallas_call(
        kernel,
        out_shape=pltpu.VMEM((ROWS, WIDTH), BF16),
        in_specs=[anywhere] * 15,
        out_specs=vmem,
        scratch_shapes=[
            pltpu.VMEM((1, 128), F32),
            pltpu.VMEM((1, WIDTH), F32),
            pltpu.VMEM((2, ROWS), I32),
            pltpu.VMEM((1, ROWS), F32),
            pltpu.VMEM((2, ROWS), F32),
            pltpu.VMEM((SEG, 256), BF16),
            pltpu.VMEM((SEG, 256), BF16),
            pltpu.VMEM((SEG, half), BF16),
            pltpu.VMEM((SEG, half), BF16),
            pltpu.VMEM((SEG, 256), BF16),
            pltpu.VMEM((ROWS, WIDTH), BF16),
            pltpu.VMEM((2 * half, WIDTH), BF16),
            pltpu.VMEM((WIDTH, HIDDEN), BF16),
            pltpu.VMEM((WIDTH, HIDDEN), BF16),
            pltpu.VMEM((HIDDEN, WIDTH), BF16),
            pltpu.VMEM((SEG, 256), F32),
            pltpu.VMEM((2, SEG, 256), BF16),
            pltpu.VMEM((SEG, half), F32),
            pltpu.VMEM((SEG, half), F32),
            pltpu.VMEM((PAIRS, SEG, 256), BF16),
            pltpu.VMEM((PAIRS, ROWS, 256), BF16),
            pltpu.VMEM((3, PIECES, 4, PIECE + 16, 128), BF16),
            pltpu.VMEM((SLOTS, ROWS), BF16),
            pltpu.VMEM((PARTS, 2 * ROWS, PART), BF16),
            pltpu.VMEM((ROWS, WIDTH), BF16),
            pltpu.VMEM((ROWS, WIDTH), F32),
            pltpu.VMEM((PART, WIDTH), BF16),
            pltpu.VMEM(((PART + 2) * PITCH, 128), F32),
            tiles,
            tiles,
            pltpu.VMEM((PART, HIDDEN), BF16),
            tiles,
            tiles,
            dma((11,)), dma((4,)),
            dma, dma((3, PIECES)),
            dma((PAIRS,)), dma((PAIRS,)), dma, dma((PARTS,)), dma, dma((PARTS,)),
        ],
        compiler_params=pltpu.CompilerParams(
            collective_id=0, has_side_effects=True, vmem_limit_bytes=56 * 2**20
        ),
    )(
        residual, queries, key_rows, value_rows, out_gate, gate_logits,
        head_gain.reshape(1, 128), out_weight, norm_gain.reshape(1, WIDTH),
        routes.T, group_score.reshape(1, ROWS), expert_score.T, gate_weight, up_weight, down_weight,
    )


def solution(mesh):
    torus = Mesh(mesh.devices.reshape(4, 4, 4, mesh.shape["tp"]), AXES)
    both = P(AXES)
    in_specs = (
        P(AXES, None),
        P(SP, "tp"), P(SP, "tp"), P(SP, "tp"), P(SP, "tp"), P(SP, "tp"),
        P(), P(), P(),
        P(AXES, None), both, P(AXES, None),
        P(AXES, None, None), P(AXES, None, None), P(AXES, None, None),
    )
    return jax.shard_map(
        local, mesh=torus, in_specs=in_specs, out_specs=P(AXES, None), check_vma=False
    )
```
